32 devices in a mesh: sp: 8 (over z, x), tp: 4 (over y, core).
Axes of the slice: x: 2, y: 2, z: 4, core: 2. Of those that a mesh axis runs over, the one named last changes fastest.
Arguments:
- probe_vectors: bfloat16 [1024, 2048], P('sp', 'tp'), may hold values from -6 to 6
- address_vectors: bfloat16 [1024, 2048], P('sp', 'tp'), may hold values from -6 to 6
- content_vectors: bfloat16 [1024, 2048], P('sp', 'tp'), may hold values from -6 to 6
- storage_raw_signal: float32 [16, 1024], P('tp', 'sp'), may hold values from -8 to 4
- fade_raw_signal: float32 [16, 1024], P('tp', 'sp'), may hold values from -6 to 6
- channel_fade_exponent: float32 [16], P('tp'), may hold values from -9 to 0
- extra_fade_amount: float32 [16, 1024], P('tp', 'sp'), may hold values from -1 to 0
- sequence_label: int32 [1024], P('sp'), may hold values from 0 to 2, never falling along the last dimension, each value on 1 to 768 neighbouring positions
- exit_valve_raw_signal: bfloat16 [1024, 2048], P('sp', 'tp'), may hold values from -6 to 6
- final_projection_matrix: bfloat16 [2048, 2048], P('tp'), may hold values from -0.125 to 0.125
- incoming_rows_matrix: bfloat16 [1024, 2048], P('sp', 'tp'), may hold values from -48 to 48
- initial_rescale_factor: float32 [2048], P('tp'), may hold values from 0 to 3
- specialist_picks: int32 [1024, 2], P('sp'), may hold values from 0 to 7, all different within a row; in each aligned block of 128 rows (0 to 127, 128 to 255, ...) at most 36 rows name the same one
- picked_specialist_share: bfloat16 [1024, 2], P('sp'), may hold values from 0.29882812 to 1.1953125
- specialist_valve_matrix: bfloat16 [8, 2048, 4096], P('sp', None, 'tp'), may hold values from -0.125 to 0.125
- specialist_raising_matrix: bfloat16 [8, 2048, 4096], P('sp', None, 'tp'), may hold values from -0.125 to 0.125
- specialist_lowering_matrix: bfloat16 [8, 4096, 2048], P('sp', 'tp'), may hold values from -0.09375 to 0.09375
- common_valve_matrix: bfloat16 [2048, 512], P(None, 'tp'), may hold values from -0.125 to 0.125
- common_raising_matrix: bfloat16 [2048, 512], P(None, 'tp'), may hold values from -0.125 to 0.125
- common_lowering_matrix: bfloat16 [512, 2048], P('tp'), may hold values from -0.25 to 0.25
- latter_rescale_factor: float32 [2048], P('tp'), may hold values from 0.1 to 1.9
Outputs:
- result: bfloat16 [1024, 2048], P('sp', 'tp')
The draws below stay inside these ranges and needn't reach their ends.
Inputs may be any that keep to these rules, and one draw needn't show every extreme that they name: `sequence_label`: document numbers never fall; a document has 1 to 768 positions, one exactly 768. `specialist_picks`: each row names 2 different experts; among the rows of one index of sp no expert is named more than 36 times, a bound that some block reaches.
All inputs are finite; a program needn't handle non-finite values.
Results may differ from the reference program's by a relative error of at most 0.018.
Values may be sent and summed in bfloat16 or wider, within the bound.
A program may use at most 64 MiB of HBM per device.

```python
import math
import jax
import jax.numpy as jnp
import numpy as np
from jax import lax

D = 2048
H = 16
DK = 128
DV = 128
BLOCK = 64
FF = 4096
SF = 512
TOP = 2
TOK_DEV = 128
TOKENS = 1024
EXPERTS = 8
CAP = 36
DOC_SPAN = 768
DOCS = 3
N_SP = 8
N_TP = 4


def slow_heads(key):
    share = 0.5
    return jax.random.bernoulli(jax.random.fold_in(key, 11), share, (H,))


def draw_channel_fade_exponent(key, part):
    slower = slow_heads(key)
    jitter = jax.random.uniform(jax.random.fold_in(key, 12), (H,), jnp.float32, -0.3, 0.3)
    slow_rate = math.log(0.6 / DOC_SPAN)
    fast_rate = math.log(2.0 / BLOCK)
    return jnp.where(slower, slow_rate, fast_rate) + jitter


def draw_storage_raw_signal(key, part):
    slower = slow_heads(key)
    base_level = jnp.where(slower, math.log(0.3 * DK / DOC_SPAN), 0.0)
    noise = jnp.clip(jax.random.normal(jax.random.fold_in(key, 13), (H, TOKENS), jnp.float32), -4.0, 4.0)
    return base_level[:, None] + noise


def draw_fade_raw_signal(key, part):
    offsets = jax.random.uniform(jax.random.fold_in(key, 14), (TOKENS // TOK_DEV,), jnp.float32, -1.2, 1.2)
    spread_out = jnp.repeat(offsets, TOK_DEV)
    noise = jnp.clip(jax.random.normal(jax.random.fold_in(key, 15), (H, TOKENS), jnp.float32), -4.0, 4.0)
    return noise + spread_out[None, :]


def draw_extra_fade_amount(key, part):
    places = jax.random.randint(jax.random.fold_in(key, 16), (H, 12), 0, TOKENS)
    depths = jax.random.uniform(jax.random.fold_in(key, 17), (H, 12), jnp.float32, math.log(0.5), math.log(0.6))
    positions = jnp.arange(TOKENS, dtype=jnp.int32)
    hits = (positions[None, None, :] == places[:, :, None]).astype(jnp.float32)
    return jnp.min(hits * depths[:, :, None], 1)


def draw_incoming_rows_matrix(key, part):
    ramp = jnp.exp(jnp.linspace(math.log(0.5), math.log(1.5), D)) * jax.random.uniform(jax.random.fold_in(key, 18), (D,), jnp.float32, 0.7, 1.3)
    row_scale = jnp.exp(jax.random.uniform(jax.random.fold_in(key, 19), (TOKENS, 1), jnp.float32, 0.0, math.log(4.0)))
    base_draw = jnp.clip(jax.random.normal(jax.random.fold_in(key, 21), (TOKENS, D), jnp.float32), -5.0, 5.0)
    return (base_draw * ramp[None, :] * row_scale).astype(jnp.bfloat16)


def draw_initial_rescale_factor(key, part):
    ramp = jnp.exp(jnp.linspace(math.log(0.6), math.log(1.8), D))
    noise = jax.random.uniform(jax.random.fold_in(key, 22), (D,), jnp.float32, 0.8, 1.2)
    return ramp * noise


def block_levels(rng, extent, pieces, smallest, top_value):
    level = 1.0
    for dim, shards_of in pieces:
        draws = jax.random.uniform(jax.random.fold_in(jax.random.fold_in(rng, 6), dim), (shards_of,), jnp.float32, smallest / len(pieces), top_value / len(pieces))
        level = level * jnp.repeat(jnp.exp(draws), extent[dim] // shards_of).reshape((-1,) + (1,) * (len(extent) - 1 - dim))
    return level


def length_profile(number_of, total, limit, skew):
    portions = [(1 << 20) // math.isqrt(grade ** skew) + 1 for grade in range(2, number_of + 1)]
    spare, counts = total - limit - (number_of - 1), [1] * (number_of - 1)
    while spare > 0:
        candidates = [i for i in range(number_of - 1) if counts[i] < limit]
        whole, left = sum([portions[i] for i in candidates]), spare
        for i in candidates:
            extra = min(limit - counts[i], max(1, left * portions[i] // whole), spare)
            counts[i] = counts[i] + extra
            spare = spare - extra
    return np.array([limit] + counts)


def uneven(own_key, amount, total, most, skew):
    if amount == 2:
        one = jax.random.randint(own_key, (), max(1, total - most), min(most, total - 1) + 1)
        return jnp.stack([one, total - one])
    lengths = jnp.asarray(length_profile(amount, total, most, skew), jnp.int32)
    pairs = (amount - 1) // 2
    donor, sink = lengths[1:1 + 2 * pairs:2], lengths[2:2 + 2 * pairs:2]
    room = jnp.minimum(donor - 1, most - sink)
    shifted = jax.random.randint(jax.random.fold_in(own_key, 1), (pairs,), 0, 1 << 20) % (room + 1)
    lengths = lengths.at[1:1 + 2 * pairs:2].set(donor - shifted).at[2:2 + 2 * pairs:2].set(sink + shifted)
    return lengths[jax.random.permutation(jax.random.fold_in(own_key, 2), amount)]


def assign_block(own_key, own, number, rows, count, top, reach, skew):
    sequence = jax.random.permutation(own_key, count)
    packed, usual = load_shares(count, rows * top, reach, skew, True), load_shares(count, rows * top, reach, skew, False)
    places = jnp.arange(count)

    def named(tallies, turn):
        used = int((tallies > 0).sum())
        fixed = max(1, used // 4)
        shifted = fixed + (places - fixed + turn * (used - fixed)) % max(1, count - fixed)
        return jnp.zeros((count,), jnp.int32).at[sequence[jnp.where(places < fixed, places, shifted)]].set(jnp.asarray(tallies, jnp.int32))

    tallies = jnp.where(number % 4 == 0, named(packed, number // 4), named(usual, number - number // 4 - 1))
    mixed = jax.random.permutation(jax.random.fold_in(own, 3), count)
    donor, sink = mixed[0:count // 2 * 2:2], mixed[1:count // 2 * 2:2]
    slack = jnp.minimum(tallies[donor] - 1, reach - tallies[sink]) // 2
    slack = jnp.where((donor == sequence[0]) | (sink == sequence[0]) | (tallies[sink] == 0), 0, jnp.maximum(slack, 0))
    shifted = jax.random.randint(jax.random.fold_in(own, 4), (count // 2,), 0, 1 << 20) % (slack + 1)
    tallies = tallies.at[donor].add(-shifted).at[sink].add(shifted)
    members = jnp.searchsorted(jnp.cumsum(tallies), jnp.arange(rows * top), side="right").astype(jnp.int32)
    table = members.reshape(top, rows).T
    table = table[jax.random.permutation(jax.random.fold_in(own, 1), rows)]
    turn = jax.random.randint(jax.random.fold_in(own, 2), (rows, 1), 0, top)
    return jnp.take_along_axis(table, (jnp.arange(top)[None, :] + turn) % top, axis=1)


def load_shares(count, total, limit, lean, full):
    weights = [(1 << 20) // math.isqrt(grade ** lean) + 1 for grade in range(1, count + 1)]
    largest = limit if full else min(limit, max(-(-total // count), total * weights[0] // sum(weights)))
    least = 1 if total - largest >= count - 1 else 0
    holding, rest = [largest] + [least] * (count - 1), total - largest - least * (count - 1)
    while rest > 0:
        free = [i for i in range(1, count) if holding[i] < largest] or [i for i in range(1, count) if holding[i] < limit]
        pool, remaining = sum([weights[i] for i in free]), rest
        for i in free:
            addition = min(limit - holding[i], max(1, remaining * weights[i] // pool), rest)
            holding[i] = holding[i] + addition
            rest = rest - addition
    return np.array(holding)


def scatter_about(key, shape, width, most, shards=(), kind=jnp.bfloat16):
    drawn = width * jax.random.normal(key, shape, jnp.float32)
    if shards:
        drawn = drawn * block_levels(key, shape, shards, -0.22, 0.18)
    return jnp.clip(drawn, -most, most).astype(kind)


def setup_inputs(seed: int = 0) -> dict:
    splits = jax.random.split(jax.random.key(seed), 22)
    probe_vectors = scatter_about(splits[0], (TOKENS, H * DK), 1.0, 6.0, ((0, 8), (1, 4)))
    address_vectors = scatter_about(splits[1], (TOKENS, H * DK), 1.0, 6.0, ((0, 8), (1, 4)))
    content_vectors = scatter_about(splits[2], (TOKENS, H * DV), 1.0, 6.0, ((0, 8), (1, 4)))
    storage_raw_signal = draw_storage_raw_signal(jax.random.fold_in(splits[21], 71), 0)
    fade_raw_signal = draw_fade_raw_signal(jax.random.fold_in(splits[21], 71), 0)
    channel_fade_exponent = draw_channel_fade_exponent(jax.random.fold_in(splits[21], 71), 0)
    extra_fade_amount = draw_extra_fade_amount(jax.random.fold_in(splits[21], 71), 0)
    sequence_label = jnp.searchsorted(jnp.cumsum(uneven(splits[7], DOCS, TOKENS, DOC_SPAN, 1)), jnp.arange(TOKENS), side="right").astype(jnp.int32)
    exit_valve_raw_signal = scatter_about(splits[8], (TOKENS, H * DV), 1.0, 6.0, ((0, 8), (1, 4)))
    final_projection_matrix = scatter_about(splits[9], (H * DV, D), (H * DV) ** -0.5, 0.125, ((0, 4),))
    incoming_rows_matrix = draw_incoming_rows_matrix(jax.random.fold_in(splits[21], 71), 0)
    initial_rescale_factor = draw_initial_rescale_factor(jax.random.fold_in(splits[21], 71), 0)
    specialist_picks_keys = jax.random.split(jax.random.fold_in(splits[12], 1), TOKENS // TOK_DEV)
    specialist_picks_turns = jax.random.permutation(jax.random.fold_in(splits[12], 3), TOKENS // TOK_DEV)
    specialist_picks = jax.vmap(lambda own, number: assign_block(jax.random.fold_in(splits[12], 2), own, number, TOK_DEV, EXPERTS, TOP, CAP, 1))(specialist_picks_keys, specialist_picks_turns).reshape((TOKENS, TOP))
    picked_specialist_share = jnp.clip(0.29882812 + 0.8964844 * jax.random.uniform(splits[13], (TOKENS, TOP), jnp.float32) ** block_levels(splits[13], (TOKENS, TOP), ((0, 8),), -0.2, 0.2), 0.29882812, 1.1953125).astype(jnp.bfloat16)
    specialist_valve_matrix = scatter_about(splits[14], (EXPERTS, D, FF), D ** -0.5, 0.125, ((0, 8), (2, 4)))
    specialist_raising_matrix = scatter_about(splits[15], (EXPERTS, D, FF), D ** -0.5, 0.125, ((0, 8), (2, 4)))
    specialist_lowering_matrix = scatter_about(splits[16], (EXPERTS, FF, D), FF ** -0.5, 0.09375, ((0, 8), (1, 4)))
    common_valve_matrix = scatter_about(splits[17], (D, SF), D ** -0.5, 0.125, ((1, 4),))
    common_raising_matrix = scatter_about(splits[18], (D, SF), D ** -0.5, 0.125, ((1, 4),))
    common_lowering_matrix = scatter_about(splits[19], (SF, D), SF ** -0.5, 0.25, ((0, 4),))
    latter_rescale_factor = jnp.clip(1.0 + 0.18 * jax.random.normal(splits[20], (D,), jnp.float32), 0.1, 1.9)
    return dict(probe_vectors=probe_vectors, address_vectors=address_vectors, content_vectors=content_vectors, storage_raw_signal=storage_raw_signal, fade_raw_signal=fade_raw_signal, channel_fade_exponent=channel_fade_exponent, extra_fade_amount=extra_fade_amount, sequence_label=sequence_label, exit_valve_raw_signal=exit_valve_raw_signal, final_projection_matrix=final_projection_matrix, incoming_rows_matrix=incoming_rows_matrix, initial_rescale_factor=initial_rescale_factor, specialist_picks=specialist_picks, picked_specialist_share=picked_specialist_share, specialist_valve_matrix=specialist_valve_matrix, specialist_raising_matrix=specialist_raising_matrix, specialist_lowering_matrix=specialist_lowering_matrix, common_valve_matrix=common_valve_matrix, common_raising_matrix=common_raising_matrix, common_lowering_matrix=common_lowering_matrix, latter_rescale_factor=latter_rescale_factor)


HIGH = lax.Precision.HIGHEST
ALPHA = 2.0 ** 0.25

def stored_value(array):
    return lax.optimization_barrier(array.astype(jnp.bfloat16)).astype(jnp.float32)

def unit_rows(array):
    return array * lax.rsqrt(lax.optimization_barrier(jnp.sum(array * array, -1, keepdims=True)) + 1e-06)

def layer_norm(summed, gain):
    row_mean = lax.optimization_barrier(jnp.mean(summed, -1, keepdims=True))
    centred = summed - row_mean
    row_var = lax.optimization_barrier(jnp.mean(centred * centred, -1, keepdims=True))
    return centred * lax.rsqrt(row_var + 1e-05) * gain

def correction_memory_layer(probe_vectors, address_vectors, content_vectors, storage_raw_signal, fade_raw_signal, channel_fade_exponent, extra_fade_amount, sequence_label):
    query_unit = unit_rows(probe_vectors.astype(jnp.float32).reshape(TOKENS, H, DK)) * DK ** (-0.5)
    key_unit = unit_rows(address_vectors.astype(jnp.float32).reshape(TOKENS, H, DK))
    value_rows = content_vectors.astype(jnp.float32).reshape(TOKENS, H, DV)
    write_gate = jax.nn.sigmoid(storage_raw_signal).T
    fade_factor = jnp.exp(extra_fade_amount - jnp.exp(channel_fade_exponent)[:, None] * jax.nn.softplus(fade_raw_signal)).T
    prior = jnp.concatenate([sequence_label[:1], sequence_label[:-1]])
    keep_state = (sequence_label == prior).astype(jnp.float32)

    def advance(carry_state, inputs):
        query_t, key_t, value_t, write_t, decay_t, keep_t = inputs
        carry_state = carry_state * keep_t
        read_back = jnp.einsum('hd,hde->he', key_t, carry_state, precision=HIGH)
        erased = carry_state - write_t[:, None, None] * key_t[:, :, None] * read_back[:, None, :]
        carry_state = decay_t[:, None, None] * erased + write_t[:, None, None] * key_t[:, :, None] * value_t[:, None, :]
        output_t = jnp.einsum('hd,hde->he', query_t, carry_state, precision=HIGH)
        return (carry_state, output_t)
    initial = jnp.zeros((H, DK, DV), jnp.float32)
    unused, memory_layer_result = lax.scan(advance, initial, (query_unit, key_unit, value_rows, write_gate, fade_factor, keep_state))
    return memory_layer_result

def expert_layer(middle, specialist_picks, picked_specialist_share, specialist_valve_matrix, specialist_raising_matrix, specialist_lowering_matrix, common_valve_matrix, common_raising_matrix, common_lowering_matrix):
    picks = TOKENS * TOP
    slots = N_SP * CAP
    flat_routes = specialist_picks.reshape(picks)
    flat_weights = picked_specialist_share.reshape(picks).astype(jnp.float32)
    group_ff = FF // N_TP
    group_sf = SF // N_TP

    def visit(total, expert):
        chosen = flat_routes == expert
        rank_in = jnp.cumsum(chosen.astype(jnp.int32)) - 1
        target = jnp.where(chosen, rank_in, slots)
        owner = jnp.full((slots,), picks, jnp.int32).at[target].set(jnp.arange(picks, dtype=jnp.int32), mode='drop')
        live = (owner < picks).astype(jnp.float32)
        safe_owner = jnp.minimum(owner, picks - 1)
        source_row = safe_owner // TOP
        shared_flag = (safe_owner % TOP == 0).astype(jnp.float32) * live
        weight_e = flat_weights[safe_owner] * live
        inputs_e = middle[source_row]
        gate_e = jnp.dot(inputs_e, specialist_valve_matrix[expert], preferred_element_type=jnp.float32)
        up_e = jnp.dot(inputs_e, specialist_raising_matrix[expert], preferred_element_type=jnp.float32)
        hidden_e = (jax.nn.silu(gate_e) * up_e * weight_e[:, None]).astype(jnp.bfloat16)
        shared_g = jnp.dot(inputs_e, common_valve_matrix, preferred_element_type=jnp.float32)
        shared_u = jnp.dot(inputs_e, common_raising_matrix, preferred_element_type=jnp.float32)
        shared_hidden = (jax.nn.silu(shared_g) * shared_u * shared_flag[:, None]).astype(jnp.bfloat16)
        down_e = specialist_lowering_matrix[expert]
        summed = jnp.zeros((slots, D), jnp.float32)
        for group in range(N_TP):
            term = jnp.dot(hidden_e[:, group * group_ff:(group + 1) * group_ff], down_e[group * group_ff:(group + 1) * group_ff], preferred_element_type=jnp.float32)
            term = term + jnp.dot(shared_hidden[:, group * group_sf:(group + 1) * group_sf], common_lowering_matrix[group * group_sf:(group + 1) * group_sf], preferred_element_type=jnp.float32)
            summed = summed + stored_value(term)
        route_out = stored_value(summed)
        total = total.at[source_row].add(route_out * live[:, None])
        return (total, None)
    start = jnp.zeros((TOKENS, D), jnp.float32)
    mixture, unused = lax.scan(visit, start, jnp.arange(EXPERTS, dtype=jnp.int32))
    return mixture

def reference(probe_vectors, address_vectors, content_vectors, storage_raw_signal, fade_raw_signal, channel_fade_exponent, extra_fade_amount, sequence_label, exit_valve_raw_signal, final_projection_matrix, incoming_rows_matrix, initial_rescale_factor, specialist_picks, picked_specialist_share, specialist_valve_matrix, specialist_raising_matrix, specialist_lowering_matrix, common_valve_matrix, common_raising_matrix, common_lowering_matrix, latter_rescale_factor):
    memory_layer_result = correction_memory_layer(probe_vectors, address_vectors, content_vectors, storage_raw_signal, fade_raw_signal, channel_fade_exponent, extra_fade_amount, sequence_label)
    scaled = memory_layer_result * lax.rsqrt(lax.optimization_barrier(jnp.mean(memory_layer_result * memory_layer_result, -1, keepdims=True)) + 1e-06)
    heads_out = (scaled.reshape(TOKENS, H * DV) * jax.nn.silu(exit_valve_raw_signal.astype(jnp.float32))).astype(jnp.bfloat16)
    group_rows = H * DV // N_TP
    projected = jnp.zeros((TOKENS, D), jnp.float32)
    for group in range(N_TP):
        term = jnp.dot(heads_out[:, group * group_rows:(group + 1) * group_rows], final_projection_matrix[group * group_rows:(group + 1) * group_rows], preferred_element_type=jnp.float32)
        projected = projected + stored_value(term)
    first_sum = ALPHA * incoming_rows_matrix.astype(jnp.float32) + projected
    middle = layer_norm(first_sum, initial_rescale_factor).astype(jnp.bfloat16)
    mixture = expert_layer(middle, specialist_picks, picked_specialist_share, specialist_valve_matrix, specialist_raising_matrix, specialist_lowering_matrix, common_valve_matrix, common_raising_matrix, common_lowering_matrix)
    second_sum = ALPHA * middle.astype(jnp.float32) + mixture
    return layer_norm(second_sum, latter_rescale_factor).astype(jnp.bfloat16)
```

```python
import functools
from types import SimpleNamespace

import jax
import jax.numpy as jnp
from jax import lax
from jax.experimental import pallas as pl
from jax.experimental.pallas import tpu as pltpu
from jax.sharding import PartitionSpec as P

DK = 128
DV = 128
DOC_SPAN = 768
GROUP = 4

ALPHA = 2.0**0.25
MESH = pl.DeviceIdType.MESH
F32, BF16 = jnp.float32, jnp.bfloat16


def scan_plan(n, reach):
    hops = [1]
    covered = 1
    if reach > 1 and n > 2:
        hops.append(2)
        covered = 3
        while covered < min(reach, n - 1):
            hops.append(covered)
            covered = 2 * covered
    return hops


def hop_order(n):
    order = [0]
    for near in range(1, n // 2 + 1):
        order.append(near)
        if n - near != near:
            order.append(n - near)
    return order


def dot(left, right):
    return jnp.dot(left, right, preferred_element_type=F32)


def dot_nt(left, right):
    return lax.dot_general(left, right, (((1,), (1,)), ((), ())), preferred_element_type=F32)


def dot_tn(left, right):
    return lax.dot_general(left, right, (((0,), (0,)), ((), ())), preferred_element_type=F32)


def iota(shape, dim):
    return lax.broadcasted_iota(jnp.int32, shape, dim)


def row_stats(array):
    lane = iota((array.shape[0], 128), 1)
    total = jnp.sum(array, -1, keepdims=True)
    square = jnp.sum(array * array, -1, keepdims=True)
    return jnp.where(lane == 0, total, jnp.where(lane == 1, square, 0.0)).T[:8]


def columns_of(rows):
    return jnp.concatenate([rows] * (128 // rows.shape[0]), 0).T


def whole_kernel(plan, *refs):
    r = SimpleNamespace(**dict(zip(plan.names, refs)))
    ns, nt, cap, pad = plan.ns, plan.nt, plan.cap, plan.pad
    size, held, hops = plan.size, plan.held, plan.hops
    order = hop_order(ns)
    groups_all = ns // size
    sp, tp = lax.axis_index("sp"), lax.axis_index("tp")
    chips = nt // 2
    chip, core = tp // 2, lax.rem(tp, 2)
    partner = tp + 1 - 2 * core
    member, group = lax.rem(sp, size), sp // size
    first = group * size
    out_ref = r.out
    tokens, width = out_ref.shape
    heads = r.storage.shape[0]
    span = held * DK
    units, narrow = r.wv_hbm.shape[2], r.cv_hbm.shape[1]
    joint = narrow % 128 == 0
    experts = ns

    hid_w = r.wd
    pairs = [
        (r.wo_hbm, r.wo),
        (r.wv_hbm.at[0], r.wv),
        (r.wr_hbm.at[0], r.wr),
    ]
    if joint:
        pairs += [
            (r.cv_hbm, r.cvr.at[:, :narrow]),
            (r.cr_hbm, r.cvr.at[:, narrow:]),
        ]
    else:
        pairs += [(r.cv_hbm, r.cvr.at[0]), (r.cr_hbm, r.cvr.at[1])]
    pairs += [(r.wd_hbm.at[0], hid_w.at[:units]), (r.cd_hbm, hid_w.at[units:])]
    loads = [
        pltpu.make_async_copy(source, target, r.weight_sem.at[i])
        for i, (source, target) in enumerate(pairs)
    ]
    barrier = pltpu.get_barrier_semaphore()
    for hop in range(1, ns):
        pl.semaphore_signal(
            barrier, inc=1, device_id={"sp": lax.rem(sp + hop, ns)}, device_id_type=MESH
        )
    for hop in range(1, nt):
        pl.semaphore_signal(
            barrier, inc=1, device_id={"tp": lax.rem(tp + hop, nt)}, device_id_type=MESH
        )
    for load in loads:
        load.start()

    row, col = iota((tokens, tokens), 0), iota((tokens, tokens), 1)
    upper = (row <= col).astype(BF16)
    rate = jnp.exp(r.fade_exp[...])
    eye_h = iota((heads, heads), 0) == iota((heads, heads), 1)
    rate = jnp.sum(jnp.where(eye_h, rate, 0.0), 1, keepdims=True)
    decay = r.extra[...] - rate * jnp.log(1.0 + jnp.exp(r.fade[...]))
    write = 1.0 / (1.0 + jnp.exp(-r.storage[...]))
    high = decay.astype(BF16)
    rest = decay - high.astype(F32)
    middle_part = rest.astype(BF16)
    low = (rest - middle_part.astype(F32)).astype(BF16)
    cumulative = dot(high, upper) + dot(middle_part, upper) + dot(low, upper)
    label = r.label[...].astype(F32)
    slot = iota((8, tokens), 0)
    scal_out, scal_in = r.scal_out, r.scal_in
    for h in range(heads):
        tile = jnp.where(slot == 0, write[h : h + 1], 0.0)
        tile = jnp.where(slot == 1, cumulative[h : h + 1], tile)
        scal_out[h] = jnp.where(slot == 2, label, tile)
    r.gain_out[...] = jnp.broadcast_to(r.gain[...], r.gain_out.shape)
    pl.semaphore_wait(barrier, ns - 1 + nt - 1)
    waits = []

    def send(source, target, sems, place, where):
        copy = pltpu.make_async_remote_copy(
            src_ref=source,
            dst_ref=target,
            send_sem=sems.at[(0,) + place],
            recv_sem=sems.at[(1,) + place],
            device_id=where,
            device_id_type=MESH,
        )
        copy.start()
        waits.append(copy)
        return copy

    def part_of(ref, which):
        return ref.at[:, pl.ds(pl.multiple_of(which * span, 128), span)]

    swaps = {}
    for index, name in enumerate(("scal", "keys", "values", "queries", "gate")):
        for p in range(1, size):
            other = lax.rem(member + p, size)
            if name == "scal":
                source, target = scal_out.at[pl.ds(other * held, held)], scal_in.at[member]
            else:
                source, target = part_of(getattr(r, name), other), getattr(r, name + "_in").at[member]
            swaps[name, p] = send(
                source, target, r.swap_sem, (index, p - 1), {"sp": first + other}
            )
    gain_in = r.gain_in
    gain_copies = [
        send(
            r.gain_out, gain_in.at[tp], r.gain_sem, (hop - 1,), {"tp": lax.rem(tp + hop, nt)}
        )
        for hop in range(1, nt)
    ]
    gain_in[tp] = r.gain_out[...]
    for h in range(held):
        scal_in[member, h] = scal_out[member * held + h]
    for name in ("keys", "values", "queries", "gate"):
        getattr(r, name + "_in")[member] = part_of(getattr(r, name), member)[...]

    r.inputs[...] = jnp.zeros_like(r.inputs)
    r.returned[...] = jnp.zeros_like(r.returned)

    pick_a = r.picks[:, 0:1].astype(F32)
    pick_b = r.picks[:, 1:2].astype(F32)
    share = r.share[...].astype(F32)
    lane = iota((tokens, 128), 1)
    lane_f = lane.astype(F32)
    member_of = ((pick_a == lane_f) | (pick_b == lane_f)).astype(F32)
    strict_low = (row > col).astype(BF16)
    ranks = dot(strict_low, member_of.astype(BF16))
    coded = ((ranks + 1.0) * member_of).astype(BF16)
    slots = experts * pad
    owner = iota((128, slots), 0)
    place = iota((128, slots), 1)
    spread = ((place >= owner * pad) & (place < owner * pad + pad)).astype(BF16)
    column = iota((8, slots), 1).astype(F32)
    expert_of = jnp.floor((column + 0.5) * (1.0 / pad))
    local = column - expert_of * pad + 1.0
    pick_t = (dot(coded, spread) == local[0:1]).astype(F32)
    r.pick_t[...] = pick_t.astype(BF16)
    r.pick[...] = pick_t.T.astype(BF16)
    facts = jnp.where(lane == 0, pick_a, 0.0)
    facts = jnp.where(lane == 1, share[:, 0:1], facts)
    facts = jnp.where(lane == 2, share[:, 1:2], facts)
    facts = jnp.where(lane == 3, 1.0, facts).T[:8].astype(BF16)
    facts = dot(facts, pick_t.astype(BF16))
    leads = facts[0:1] == expert_of[0:1]
    slot_weight = jnp.where(leads, facts[1:2], facts[2:3])
    slot_shared = jnp.where(leads, facts[3:4], 0.0)
    side_rows = jnp.where(iota((8, slots), 0) == 0, slot_weight, slot_shared)
    r.info[...] = jnp.zeros_like(r.info)
    for e in range(experts):
        r.info[e, :, 0:pad] = side_rows[:, e * pad : (e + 1) * pad]

    same = row == col
    inverse_ref, decay_ref, norm_ref = r.inverse, r.decay, r.norm

    def invert(blocks):
        coupled, inverse = [], []
        for b, h in blocks:
            keys = r.keys_in[b, :, h * DK : (h + 1) * DK]
            gram = dot_nt(keys, keys)
            tile = scal_in[b, h]
            columns = columns_of(tile)
            diagonal = jnp.where(same, gram, 0.0)
            norm_row = lax.rsqrt(jnp.sum(diagonal, 0, keepdims=True) + 1e-06)
            norm_col = lax.rsqrt(jnp.sum(diagonal, 1, keepdims=True) + 1e-06)
            gap = jnp.where(row >= col, columns[:, 1:2] - tile[1:2], 0.0)
            reach = jnp.where(
                (row >= col) & (columns[:, 2:3] == tile[2:3]), jnp.exp(gap), 0.0
            )
            decay_ref[b, h] = reach
            norm_ref[b, h] = jnp.broadcast_to(norm_row, (8, tokens))
            full = gram * (columns[:, 0:1] * norm_col) * norm_row * reach
            coupled.append(jnp.where(row > col, full, 0.0))
        step = 1
        while step < tokens:
            below = (row // step == col // step + 1) & (lax.rem(row // step, 2) == 1)
            picked = [jnp.where(below, one, 0.0) for one in coupled]
            if step == 1:
                inverse = [same.astype(F32) - one for one in picked]
            else:
                short = [one.astype(BF16) for one in inverse]
                right = [dot(a.astype(BF16), b) for a, b in zip(picked, short)]
                inverse = [
                    one - dot(a, b.astype(BF16)) for one, a, b in zip(inverse, short, right)
                ]
            step = 2 * step
        for (b, h), one in zip(blocks, inverse):
            inverse_ref[b, h] = one

    invert([(member, h) for h in range(held)])
    for name in ("scal", "keys"):
        for p in range(1, size):
            swaps[name, p].wait_recv()
    if size > 1:
        invert(
            [(lax.rem(member - p + size, size), h) for p in range(1, size) for h in range(held)]
        )
    for p in range(1, size):
        swaps["values", p].wait_recv()
    pieces = [(b, h) for b in range(size) for h in range(held)]
    facts_of, updates, steps = {}, {}, {}
    for b, h in pieces:
        tile = scal_in[b, h]
        norm_row = norm_ref[b, h][0:1]
        tile = jnp.where(slot == 3, norm_row, tile)
        columns = columns_of(tile)
        before = scal_in[b - 1, h][2:3, tokens - 1 :] if b else tile[2:3, 0:1]
        last_label, last_sum = tile[2:3, tokens - 1 :], tile[1:2, tokens - 1 :]
        growth_row = jnp.exp(tile[1:2]) * (tile[2:3] == before).astype(F32)
        growth_col = jnp.exp(columns[:, 1:2]) * (columns[:, 2:3] == before).astype(F32)
        tail = jnp.exp(last_sum - columns[:, 1:2]) * (columns[:, 2:3] == last_label).astype(F32)
        fade = jnp.exp(last_sum) * (last_label == before).astype(F32)
        inverse = inverse_ref[b, h]
        keys = r.keys_in[b, :, h * DK : (h + 1) * DK]
        values = r.values_in[b, :, h * DV : (h + 1) * DV]
        update = dot((inverse * tile[0:1]).astype(BF16), values)
        correct = dot((inverse * (tile[0:1] * norm_row * growth_row)).astype(BF16), keys)
        both = jnp.concatenate([update, correct], 1)
        updates[b, h] = both.astype(BF16)
        made = dot_tn(keys, (both * (tail * columns[:, 3:4])).astype(BF16))
        steps[b, h] = (made[:, :DV], made[:, DV:], fade)
        facts_of[b, h] = (growth_col, norm_row)
    built, landed = r.built, r.landed
    rounds = len(hops)
    entry = {}
    summary = {}
    for h in range(held):
        add, erase, fade = steps[0, h]
        carry = jnp.concatenate([jnp.where(same, fade, 0.0) - erase, add], 1)
        for b in range(1, size):
            entry[b, h] = carry.astype(BF16)
            add, erase, fade = steps[b, h]
            carry = fade * carry - dot(erase.astype(BF16), entry[b, h])
            carry = jnp.concatenate([carry[:, :DK], carry[:, DK:] + add], 1)
        summary[h] = carry

    def copy_to_group(source, target, sems, hop):
        return pltpu.make_async_remote_copy(
            src_ref=source,
            dst_ref=target,
            send_sem=sems[0],
            recv_sem=sems[1],
            device_id={"sp": lax.rem(sp + hop * size, ns)},
            device_id_type=MESH,
        )

    def scan_copy(index):
        last = index == rounds - 1
        source, target = built.at[index], landed.at[index]
        if last:
            source, target = source.at[1], target.at[1]
        sems = r.scan_sem.at[0, index], r.scan_sem.at[1, index]
        return copy_to_group(source, target, sems, hops[index])

    note = None
    if groups_all > 1:
        note = copy_to_group(
            scal_in.at[size - 1, 0],
            r.label_note,
            (r.note_sem.at[0], r.note_sem.at[1]),
            1,
        )
        note.start()
        for h in range(held):
            built[0, 1, h] = summary[h][:, DK:].astype(BF16)
    single = rounds == 1
    if groups_all > 1 and single:

        @pl.when(group + hops[0] < groups_all)
        def _():
            scan_copy(0).start()

    for p in range(1, size):
        swaps["queries", p].wait_recv()
    for b, h in pieces:
        growth_col, norm_row = facts_of[b, h]
        keys = r.keys_in[b, :, h * DK : (h + 1) * DK]
        queries = r.queries_in[b, :, h * DK : (h + 1) * DK]
        wide = queries.astype(F32)
        scale = lax.rsqrt(jnp.sum(wide * wide, 1, keepdims=True) + 1e-06) * DK ** (-0.5)
        scores = (dot_nt(queries, keys) * scale * norm_row * decay_ref[b, h]).astype(BF16)
        seen = dot(scores, updates[b, h])
        grown = wide * (scale * growth_col) - seen[:, DV:]
        rows_here = pl.ds(b * tokens, tokens)
        if b:
            carried = dot(grown.astype(BF16), entry[b, h])
            r.reader[h, rows_here] = carried[:, :DK].astype(BF16)
            r.partial[h, rows_here] = seen[:, :DV] + carried[:, DK:]
        else:
            r.reader[h, rows_here] = grown.astype(BF16)
            r.partial[h, rows_here] = seen[:, :DV]
    incoming = None
    if groups_all > 1:
        note.wait_recv()
        joined = (r.label_note[2:3, tokens - 1 :] == scal_in[0, 0][2:3, 0:1]) & (group > 0)
        joined = joined.astype(F32)
        window = None
        if not single:
            for h in range(held):
                built[0, 0, h] = (summary[h][:, :DK] * joined).astype(BF16)
        for index, hop in enumerate(hops):
            last = index == rounds - 1
            if not single:

                @pl.when(group + hop < groups_all)
                def _():
                    scan_copy(index).start()

            @pl.when(group >= hop)
            def _():
                scan_copy(index).wait_recv()

            @pl.when(group < hop)
            def _():
                landed[index] = jnp.zeros_like(landed[index])

            got = landed.at[index]
            if index == 0:
                if last:
                    incoming = [got[1, h].astype(F32) * joined for h in range(held)]
                else:
                    for h in range(held):
                        built[1, 0, h] = dot(built[0, 0, h], got[0, h]).astype(BF16)
                        built[1, 1, h] = (
                            dot(built[0, 0, h], got[1, h]) + built[0, 1, h].astype(F32)
                        ).astype(BF16)
                window = got
            else:
                shifts = [
                    dot(window[0, h], got[1, h]) + window[1, h].astype(F32) for h in range(held)
                ]
                if last:
                    incoming = [one * joined for one in shifts]
                else:
                    for h in range(held):
                        built[index + 1, 0, h] = dot(window[0, h], got[0, h]).astype(BF16)
                        built[index + 1, 1, h] = shifts[h].astype(BF16)
                    window = built.at[index + 1]
    for p in range(1, size):
        swaps["gate", p].wait_recv()
    for h in range(held):
        mixed = r.partial[h]
        if incoming is not None:
            mixed = mixed + dot(r.reader[h], incoming[h].astype(BF16))
        mixed = mixed * lax.rsqrt(jnp.mean(mixed * mixed, -1, keepdims=True) + 1e-06)
        for b in range(size):
            gate = r.gate_in[b, :, h * DV : (h + 1) * DV].astype(F32)
            here = mixed[b * tokens : (b + 1) * tokens] * (gate / (1.0 + jnp.exp(-gate)))
            r.mixed[b, :, h * DV : (h + 1) * DV] = here.astype(BF16)
    gives = []
    for p in range(1, size):
        other = lax.rem(member + p, size)
        gives.append(
            send(
                r.mixed.at[other],
                part_of(r.heads, member),
                r.give_sem,
                (p - 1,),
                {"sp": first + other},
            )
        )
    part_of(r.heads, member)[...] = r.mixed[member]
    for copy in gives:
        copy.wait_recv()
    loads[0].wait()

    def head_block(t):
        start = pl.multiple_of(t * width, width)
        return dot(r.heads[...], r.wo[:, pl.ds(start, width)])

    far_first = list(range(1, chips)) + [0]
    head_pairs, head_across = {}, []
    for k in far_first:
        r.head_out[k] = head_block(2 * lax.rem(chip + k, chips) + 1 - core).astype(BF16)
        head_pairs[k] = send(
            r.head_out.at[k], r.head_in.at[k], r.head_sem, (k,), {"tp": partner}
        )
    for k in far_first:
        there = 2 * lax.rem(chip + k, chips) + core
        value = head_block(there)
        head_pairs[k].wait_recv()
        value = value + r.head_in[k].astype(F32)
        if k:
            r.head_yout[k - 1] = value.astype(BF16)
            head_across.append(
                send(
                    r.head_yout.at[k - 1],
                    r.head_yin.at[k - 1],
                    r.head_sem,
                    (chips + k - 1,),
                    {"tp": there},
                )
            )
    projected = value + ALPHA * r.rows[...].astype(F32)
    for k, copy in enumerate(head_across):
        copy.wait_recv()
        projected = projected + r.head_yin[k].astype(F32)

    picked = dot(r.pick[...], projected.astype(BF16)).astype(BF16)
    sbuf, gathered, infos = r.sbuf, r.gathered, r.infos
    for e in range(experts):
        sbuf[e] = picked[e * pad : e * pad + cap]
    arrivals, notes = {}, []
    for i, hop in enumerate(order):
        if hop:
            to = lax.rem(sp + hop, ns)
            arrivals[i] = send(sbuf.at[to], gathered.at[tp, i], r.sp_sem, (i - 1,), {"sp": to})
    for i, hop in enumerate(order):
        if hop:
            to = lax.rem(sp + hop, ns)
            notes.append(
                send(r.info.at[to], infos.at[i], r.info_sem, (i - 1,), {"sp": to})
            )
    gathered[tp, 0] = sbuf[sp]
    infos[0] = r.info[sp]

    def stats_start(index, summed):
        r.stat_own[index] = row_stats(summed)
        return [
            send(
                r.stat_own.at[index],
                r.stat_in.at[index, hop - 1],
                r.stat_sem,
                (index, hop - 1),
                {"tp": lax.rem(tp + hop, nt)},
            )
            for hop in range(1, nt)
        ]

    def stats_end(index, copies, summed, gain):
        total = r.stat_own[index]
        for hop in range(1, nt):
            copies[hop - 1].wait_recv()
            total = total + r.stat_in[index, hop - 1]
        total = columns_of(total / (width * nt))
        mean, square = total[:, 0:1], total[:, 1:2]
        return (summed - mean) * lax.rsqrt(square - mean * mean + 1e-05) * gain

    first_stats = stats_start(0, projected)
    half = ns // 2
    across, forward = {}, {}

    def arrive(c):
        for i in range(c * half, (c + 1) * half):
            if i:
                arrivals[i].wait_recv()
            mine = gathered.at[tp, i]
            for k in range(1, chips):
                across[i, k] = send(
                    mine, mine, r.y_sem, (i, k - 1),
                    {"tp": 2 * lax.rem(chip + k, chips) + core},
                )
            forward[i, 0] = send(mine, mine, r.pair_sem, (i, 0), {"tp": partner})

    def relay(c):
        for i in range(c * half, (c + 1) * half):
            for k in range(1, chips):
                across[i, k].wait_recv()
                theirs = gathered.at[2 * lax.rem(chip - k + chips, chips) + core, i]
                forward[i, k] = send(theirs, theirs, r.pair_sem, (i, k), {"tp": partner})

    def assemble(c):
        for i in range(c * half, (c + 1) * half):
            for k in range(chips):
                forward[i, k].wait_recv()
            if i:
                notes[i - 1].wait_recv()
            r.side[i * pad : (i + 1) * pad] = columns_of(infos[i])[:pad]
            blocks = [gathered[t, i].astype(F32) for t in range(nt)]
            total = functools.reduce(jnp.add, blocks)
            mean = jnp.sum(total, 1, keepdims=True) / (width * nt)
            blocks = [one - mean for one in blocks]
            square = functools.reduce(jnp.add, [one * one for one in blocks])
            scale = lax.rsqrt(jnp.sum(square, 1, keepdims=True) / (width * nt) + 1e-05)
            for t in range(nt):
                r.inputs[i * pad : i * pad + cap, t * width : (t + 1) * width] = (
                    blocks[t] * scale * gain_in[t][0:1]
                ).astype(BF16)

    tile = 256 if units % 256 == 0 else 128
    silu = jax.nn.silu

    def expert(c):
        rows_here = slice(c * half * pad, (c + 1) * half * pad)
        inputs = r.inputs
        weight_e, shared_e = r.side[rows_here, 0:1], r.side[rows_here, 1:2]
        if joint:
            both = dot(inputs[rows_here], r.cvr[...])
            gate, up = both[:, :narrow], both[:, narrow:]
        else:
            gate = dot(inputs[rows_here], r.cvr[0])
            up = dot(inputs[rows_here], r.cvr[1])
        r.hidden[rows_here, units:] = (silu(gate) * up * shared_e).astype(BF16)

        @pl.loop(0, units // tile)
        def _(i):
            cols = pl.ds(pl.multiple_of(i * tile, tile), tile)
            gate = dot(inputs[rows_here], r.wv[:, cols])
            up = dot(inputs[rows_here], r.wr[:, cols])
            r.hidden[rows_here, cols] = (silu(gate) * up * weight_e).astype(BF16)

    def part_block(c, t):
        rows_here = slice(c * half * pad, (c + 1) * half * pad)
        cols = pl.ds(pl.multiple_of(t * width, width), width)
        return dot(r.hidden[rows_here], hid_w[:, cols])

    part_pairs, part_across, backs = {}, {}, {}

    def lower(c):
        for k in far_first:
            value = part_block(c, 2 * lax.rem(chip + k, chips) + 1 - core).astype(BF16)
            for j in range(half):
                r.part_out[c, k, j] = value[j * pad : j * pad + cap]
            part_pairs[k] = send(
                r.part_out.at[c, k], r.part_in.at[c, k], r.part_sem, (c, k),
                {"tp": partner},
            )
        for k in far_first:
            there = 2 * lax.rem(chip + k, chips) + core
            value = part_block(c, there)
            part_pairs[k].wait_recv()
            for j in range(half):
                piece = value[j * pad : j * pad + cap] + r.part_in[c, k, j].astype(F32)
                if k:
                    r.part_yout[c, k - 1, j] = piece.astype(BF16)
                else:
                    r.own[c, j] = piece
            if k:
                part_across[c, k] = send(
                    r.part_yout.at[c, k - 1], r.part_yin.at[c, k - 1], r.part_sem,
                    (c, chips + k - 1), {"tp": there},
                )

    def give_back(c):
        for k in range(1, chips):
            part_across[c, k].wait_recv()
        for j in range(half):
            i = c * half + j
            piece = r.own[c, j]
            for k in range(1, chips):
                piece = piece + r.part_yin[c, k - 1, j].astype(F32)
            r.back_out[i] = piece.astype(BF16)
            if i:
                to = lax.rem(sp - order[i] + ns, ns)
                backs[i] = send(
                    r.back_out.at[i], r.back_in.at[sp], r.back_sem, (i - 1,), {"sp": to}
                )
            else:
                r.back_in[sp] = r.back_out[0]

    arrive(0)
    arrive(1)
    middle = stats_end(0, first_stats, projected, r.gain[...]).astype(BF16)
    for copy in gain_copies:
        copy.wait_recv()
    relay(0)
    for load in loads[1:5]:
        load.wait()
    assemble(0)
    expert(0)
    relay(1)
    for load in loads[5:]:
        load.wait()
    lower(0)
    assemble(1)
    expert(1)
    give_back(0)
    lower(1)
    give_back(1)
    for i in backs:
        backs[i].wait_recv()
    for j in range(ns):
        r.returned[j * pad : j * pad + cap] = r.back_in[j]
    second = ALPHA * middle.astype(F32) + dot(r.pick_t[...], r.returned[...])
    copies = stats_start(1, second)
    out_ref[...] = stats_end(1, copies, second, r.last_gain[...]).astype(out_ref.dtype)
    if groups_all > 1:
        for index, hop in enumerate(hops):

            @pl.when(group + hop < groups_all)
            def _():
                scan_copy(index).wait_send()

        note.wait_send()
    for copy in waits:
        copy.wait_send()


def shards(
    probe_vectors,
    address_vectors,
    content_vectors,
    storage_raw_signal,
    fade_raw_signal,
    channel_fade_exponent,
    extra_fade_amount,
    sequence_label,
    exit_valve_raw_signal,
    final_projection_matrix,
    incoming_rows_matrix,
    initial_rescale_factor,
    specialist_picks,
    picked_specialist_share,
    specialist_valve_matrix,
    specialist_raising_matrix,
    specialist_lowering_matrix,
    common_valve_matrix,
    common_raising_matrix,
    common_lowering_matrix,
    latter_rescale_factor,
):
    ns, nt = lax.axis_size("sp"), lax.axis_size("tp")
    tokens, width = incoming_rows_matrix.shape
    heads = storage_raw_signal.shape[0]
    experts = specialist_valve_matrix.shape[0] * ns
    top = specialist_picks.shape[1]
    cap = max(2, 9 * tokens * top // (8 * experts))
    pad = -(-cap // 16) * 16
    size = GROUP
    while heads % size or ns % size:
        size //= 2
    held = heads // size
    reach = -(-(DOC_SPAN - 1) // tokens)
    hops = scan_plan(ns // size, -(-reach // size))
    rounds = len(hops)
    units, narrow = specialist_valve_matrix.shape[2], common_valve_matrix.shape[1]
    features = width * nt
    chips = nt // 2
    across = max(chips - 1, 1)
    half = ns // 2
    swap = max(size - 1, 1)
    dma = pltpu.SemaphoreType.DMA

    def vm(*shape, dtype=BF16):
        return pltpu.VMEM(shape, dtype)

    f32 = functools.partial(vm, dtype=F32)
    operands = dict(
        queries=probe_vectors,
        keys=address_vectors,
        values=content_vectors,
        gate=exit_valve_raw_signal,
        storage=storage_raw_signal,
        fade=fade_raw_signal,
        fade_exp=channel_fade_exponent[None, :],
        extra=extra_fade_amount,
        label=sequence_label[None, :],
        rows=incoming_rows_matrix,
        gain=initial_rescale_factor[None, :],
        last_gain=latter_rescale_factor[None, :],
        picks=specialist_picks,
        share=picked_specialist_share,
    )
    weights = dict(
        wo_hbm=final_projection_matrix,
        wv_hbm=specialist_valve_matrix,
        wr_hbm=specialist_raising_matrix,
        wd_hbm=specialist_lowering_matrix,
        cv_hbm=common_valve_matrix,
        cr_hbm=common_raising_matrix,
        cd_hbm=common_lowering_matrix,
    )
    scratch = dict(
        wo=vm(*final_projection_matrix.shape),
        wv=vm(features, units),
        wr=vm(features, units),
        cvr=vm(features, 2 * narrow) if narrow % 128 == 0 else vm(2, features, narrow),
        wd=vm(units + narrow, features),
        weight_sem=dma((7,)),
        scal_out=f32(heads, 8, tokens),
        scal_in=f32(size, held, 8, tokens),
        keys_in=vm(size, tokens, held * DK),
        values_in=vm(size, tokens, held * DV),
        queries_in=vm(size, tokens, held * DK),
        gate_in=vm(size, tokens, held * DV),
        swap_sem=dma((2, 5, swap)),
        gain_out=f32(8, width),
        gain_in=f32(nt, 8, width),
        gain_sem=dma((2, nt - 1)),
        pick=vm(experts * pad, tokens),
        pick_t=vm(tokens, experts * pad),
        info=f32(experts, 8, 128),
        infos=f32(ns, 8, 128),
        info_sem=dma((2, ns - 1)),
        inverse=f32(size, held, tokens, tokens),
        decay=f32(size, held, tokens, tokens),
        norm=f32(size, held, 8, tokens),
        built=vm(rounds, 2, held, DK, DV),
        landed=vm(rounds, 2, held, DK, DV),
        scan_sem=dma((2, rounds)),
        label_note=f32(8, tokens),
        note_sem=dma((2,)),
        reader=vm(held, size * tokens, DK),
        partial=f32(held, size * tokens, DV),
        mixed=vm(size, tokens, held * DV),
        heads=vm(tokens, heads * DV),
        give_sem=dma((2, swap)),
        head_out=vm(chips, tokens, width),
        head_in=vm(chips, tokens, width),
        head_yout=vm(across, tokens, width),
        head_yin=vm(across, tokens, width),
        head_sem=dma((2, 2 * chips)),
        stat_own=f32(2, 8, tokens),
        stat_in=f32(2, nt - 1, 8, tokens),
        stat_sem=dma((2, 2, nt - 1)),
        sbuf=vm(ns, cap, width),
        gathered=vm(nt, ns, cap, width),
        sp_sem=dma((2, ns - 1)),
        y_sem=dma((2, ns, across)),
        pair_sem=dma((2, ns, chips)),
        inputs=vm(ns * pad, features),
        hidden=vm(ns * pad, units + narrow),
        side=f32(ns * pad, 128),
        part_out=vm(2, chips, half, cap, width),
        part_in=vm(2, chips, half, cap, width),
        part_yout=vm(2, across, half, cap, width),
        part_yin=vm(2, across, half, cap, width),
        part_sem=dma((2, 2, 2 * chips)),
        own=f32(2, half, cap, width),
        back_out=vm(ns, cap, width),
        back_in=vm(ns, cap, width),
        back_sem=dma((2, ns - 1)),
        returned=vm(ns * pad, width),
    )
    plan = SimpleNamespace(
        names=tuple(operands) + tuple(weights) + ("out",) + tuple(scratch),
        ns=ns,
        nt=nt,
        cap=cap,
        pad=pad,
        size=size,
        held=held,
        hops=hops,
    )
    return pl.pallas_call(
        functools.partial(whole_kernel, plan),
        out_shape=jax.ShapeDtypeStruct((tokens, width), BF16),
        in_specs=[pl.BlockSpec(memory_space=pltpu.VMEM)] * len(operands)
        + [pl.BlockSpec(memory_space=pl.ANY)] * len(weights),
        out_specs=pl.BlockSpec(memory_space=pltpu.VMEM),
        scratch_shapes=list(scratch.values()),
        compiler_params=pltpu.CompilerParams(
            collective_id=1, has_side_effects=True, vmem_limit_bytes=60 * 2**20
        ),
        name="whole_layer",
    )(*operands.values(), *weights.values())


def solution(mesh):
    placed = (
        P("sp", "tp"),
        P("sp", "tp"),
        P("sp", "tp"),
        P("tp", "sp"),
        P("tp", "sp"),
        P("tp"),
        P("tp", "sp"),
        P("sp"),
        P("sp", "tp"),
        P("tp", None),
        P("sp", "tp"),
        P("tp"),
        P("sp", None),
        P("sp", None),
        P("sp", None, "tp"),
        P("sp", None, "tp"),
        P("sp", "tp", None),
        P(None, "tp"),
        P(None, "tp"),
        P("tp", None),
        P("tp"),
    )
    return jax.shard_map(
        shards, mesh=mesh, in_specs=placed, out_specs=P("sp", "tp"), check_vma=False
    )
```

```python
import functools
from types import SimpleNamespace

import jax
import jax.numpy as jnp
from jax import lax
from jax.experimental import pallas as pl
from jax.experimental.pallas import tpu as pltpu
from jax.sharding import PartitionSpec as P

DK = 128
DV = 128
DOC_SPAN = 768
GROUP = 4

ALPHA = 2.0**0.25
MESH = pl.DeviceIdType.MESH
F32, BF16 = jnp.float32, jnp.bfloat16


def scan_plan(n, reach):
    hops = [1]
    covered = 1
    if reach > 1 and n > 2:
        hops.append(2)
        covered = 3
        while covered < min(reach, n - 1):
            hops.append(covered)
            covered = 2 * covered
    return hops


def hop_order(n):
    order = [0]
    for near in range(1, n // 2 + 1):
        order.append(near)
        if n - near != near:
            order.append(n - near)
    return order


def dot(left, right):
    return jnp.dot(left, right, preferred_element_type=F32)


def dot_nt(left, right):
    return lax.dot_general(left, right, (((1,), (1,)), ((), ())), preferred_element_type=F32)


def dot_tn(left, right):
    return lax.dot_general(left, right, (((0,), (0,)), ((), ())), preferred_element_type=F32)


def iota(shape, dim):
    return lax.broadcasted_iota(jnp.int32, shape, dim)


def row_stats(array):
    lane = iota((array.shape[0], 128), 1)
    total = jnp.sum(array, -1, keepdims=True)
    square = jnp.sum(array * array, -1, keepdims=True)
    return jnp.where(lane == 0, total, jnp.where(lane == 1, square, 0.0)).T[:8]


def columns_of(rows):
    return jnp.concatenate([rows] * (128 // rows.shape[0]), 0).T


def whole_kernel(plan, *refs):
    r = SimpleNamespace(**dict(zip(plan.names, refs)))
    ns, nt, cap, pad = plan.ns, plan.nt, plan.cap, plan.pad
    size, held, hops = plan.size, plan.held, plan.hops
    order, bounds = hop_order(ns), plan.bounds
    groups_all = ns // size
    sp, tp = lax.axis_index("sp"), lax.axis_index("tp")
    chips = nt // 2
    chip, core = tp // 2, lax.rem(tp, 2)
    partner = tp + 1 - 2 * core
    member, group = lax.rem(sp, size), sp // size
    first = group * size
    out_ref = r.out
    tokens, width = out_ref.shape
    heads = r.storage.shape[0]
    span = held * DK
    units, narrow = r.wv_hbm.shape[2], r.cv_hbm.shape[1]
    joint = narrow % 128 == 0
    experts = ns

    hid_w = r.wd
    pairs = [
        (r.wo_hbm, r.wo),
        (r.wv_hbm.at[0], r.wv),
        (r.wr_hbm.at[0], r.wr),
    ]
    if joint:
        pairs += [
            (r.cv_hbm, r.cvr.at[:, :narrow]),
            (r.cr_hbm, r.cvr.at[:, narrow:]),
        ]
    else:
        pairs += [(r.cv_hbm, r.cvr.at[0]), (r.cr_hbm, r.cvr.at[1])]
    pairs += [(r.wd_hbm.at[0], hid_w.at[:units]), (r.cd_hbm, hid_w.at[units:])]
    loads = [
        pltpu.make_async_copy(source, target, r.weight_sem.at[i])
        for i, (source, target) in enumerate(pairs)
    ]
    takes = {
        name: pltpu.make_async_copy(
            getattr(r, name + "_hbm"), getattr(r, name), r.take_sem.at[i]
        )
        for i, name in enumerate(plan.inputs)
    }
    for take in takes.values():
        take.start()

    def have(*names):
        for name in names or tuple(takes):
            takes.pop(name).wait()
    barrier = pltpu.get_barrier_semaphore()
    for hop in range(1, ns):
        pl.semaphore_signal(
            barrier, inc=1, device_id={"sp": lax.rem(sp + hop, ns)}, device_id_type=MESH
        )
    for hop in range(1, nt):
        pl.semaphore_signal(
            barrier, inc=1, device_id={"tp": lax.rem(tp + hop, nt)}, device_id_type=MESH
        )
    row, col = iota((tokens, tokens), 0), iota((tokens, tokens), 1)
    upper = (row <= col).astype(BF16)
    have("fade_exp", "extra", "fade", "storage", "label", "gain")
    rate = jnp.exp(r.fade_exp[...])
    eye_h = iota((heads, heads), 0) == iota((heads, heads), 1)
    rate = jnp.sum(jnp.where(eye_h, rate, 0.0), 1, keepdims=True)
    decay = r.extra[...] - rate * jnp.log(1.0 + jnp.exp(r.fade[...]))
    write = 1.0 / (1.0 + jnp.exp(-r.storage[...]))
    high = decay.astype(BF16)
    rest = decay - high.astype(F32)
    middle_part = rest.astype(BF16)
    low = (rest - middle_part.astype(F32)).astype(BF16)
    cumulative = dot(high, upper) + dot(middle_part, upper) + dot(low, upper)
    label = r.label[...].astype(F32)
    slot = iota((8, tokens), 0)
    scal_out, scal_in = r.scal_out, r.scal_in
    for h in range(heads):
        tile = jnp.where(slot == 0, write[h : h + 1], 0.0)
        tile = jnp.where(slot == 1, cumulative[h : h + 1], tile)
        scal_out[h] = jnp.where(slot == 2, label, tile)
    r.gain_out[...] = jnp.broadcast_to(r.gain[...], r.gain_out.shape)
    pl.semaphore_wait(barrier, ns - 1 + nt - 1)
    have()
    waits = []

    def send(source, target, sems, place, where):
        copy = pltpu.make_async_remote_copy(
            src_ref=source,
            dst_ref=target,
            send_sem=sems.at[(0,) + place],
            recv_sem=sems.at[(1,) + place],
            device_id=where,
            device_id_type=MESH,
        )
        copy.start()
        waits.append(copy)
        return copy

    def part_of(ref, which):
        return ref.at[:, pl.ds(pl.multiple_of(which * span, 128), span)]

    swaps = {}
    for index, name in enumerate(("scal", "keys", "values", "queries", "gate")):
        for p in range(1, size):
            other = lax.rem(member + p, size)
            if name == "scal":
                source, target = scal_out.at[pl.ds(other * held, held)], scal_in.at[member]
            else:
                source, target = part_of(getattr(r, name), other), getattr(r, name + "_in").at[member]
            swaps[name, p] = send(
                source, target, r.swap_sem, (index, p - 1), {"sp": first + other}
            )
    gain_in = r.gain_in
    gain_copies = [
        send(
            r.gain_out, gain_in.at[tp], r.gain_sem, (hop - 1,), {"tp": lax.rem(tp + hop, nt)}
        )
        for hop in range(1, nt)
    ]
    gain_in[tp] = r.gain_out[...]
    for h in range(held):
        scal_in[member, h] = scal_out[member * held + h]
    for name in ("keys", "values", "queries", "gate"):
        getattr(r, name + "_in")[member] = part_of(getattr(r, name), member)[...]

    for load in loads:
        load.start()
    r.inputs[...] = jnp.zeros_like(r.inputs)
    r.returned[...] = jnp.zeros_like(r.returned)

    pick_rows, share_rows = r.picks[...].astype(F32), r.share[...].astype(F32)
    fact_rows = jnp.where(slot == 0, pick_rows[0:1], 0.0)
    fact_rows = jnp.where(slot == 1, share_rows[0:1], fact_rows)
    fact_rows = jnp.where(slot == 2, share_rows[1:2], fact_rows)
    fact_rows = jnp.where(slot == 3, 1.0, fact_rows)
    pick_cols = columns_of(jnp.where(slot == 4, pick_rows[1:2], fact_rows))
    pick_a, pick_b = pick_cols[:, 0:1], pick_cols[:, 4:5]
    lane = iota((tokens, 128), 1)
    lane_f = lane.astype(F32)
    member_of = ((pick_a == lane_f) | (pick_b == lane_f)).astype(F32)
    strict_low = (row > col).astype(BF16)
    ranks = dot(strict_low, member_of.astype(BF16))
    coded = ((ranks + 1.0) * member_of).astype(BF16)
    slots = experts * pad
    owner = iota((128, slots), 0)
    place = iota((128, slots), 1)
    spread = ((place >= owner * pad) & (place < owner * pad + pad)).astype(BF16)
    column = iota((8, slots), 1).astype(F32)
    expert_of = jnp.floor((column + 0.5) * (1.0 / pad))
    local = column - expert_of * pad + 1.0
    pick_t = (dot(coded, spread) == local[0:1]).astype(F32)
    r.pick_t[...] = pick_t.astype(BF16)
    r.pick[...] = pick_t.T.astype(BF16)
    facts = dot(fact_rows.astype(BF16), pick_t.astype(BF16))
    leads = facts[0:1] == expert_of[0:1]
    slot_weight = jnp.where(leads, facts[1:2], facts[2:3])
    slot_shared = jnp.where(leads, facts[3:4], 0.0)
    side_rows = jnp.where(iota((8, slots), 0) == 0, slot_weight, slot_shared)
    r.info[...] = jnp.zeros_like(r.info)
    for e in range(experts):
        r.info[e, :, 0:pad] = side_rows[:, e * pad : (e + 1) * pad]

    infos, notes = r.infos, {}
    for i, hop in enumerate(order):
        if hop:
            to = lax.rem(sp + hop, ns)
            notes[i] = send(r.info.at[to], infos.at[i], r.info_sem, (i,), {"sp": to})
    infos[0] = r.info[sp]

    same = row == col
    inverse_ref, decay_ref, norm_ref = r.inverse, r.decay, r.norm

    def invert(blocks):
        coupled, inverse = [], []
        for b, h in blocks:
            keys = r.keys_in[b, :, h * DK : (h + 1) * DK]
            gram = dot_nt(keys, keys)
            tile = scal_in[b, h]
            columns = columns_of(tile)
            diagonal = jnp.where(same, gram, 0.0)
            norm_row = lax.rsqrt(jnp.sum(diagonal, 0, keepdims=True) + 1e-06)
            norm_col = lax.rsqrt(jnp.sum(diagonal, 1, keepdims=True) + 1e-06)
            gap = jnp.where(row >= col, columns[:, 1:2] - tile[1:2], 0.0)
            reach = jnp.where(
                (row >= col) & (columns[:, 2:3] == tile[2:3]), jnp.exp(gap), 0.0
            )
            decay_ref[b, h] = reach
            norm_ref[b, h] = jnp.broadcast_to(norm_row, (8, tokens))
            full = gram * (columns[:, 0:1] * norm_col) * norm_row * reach
            coupled.append(jnp.where(row > col, full, 0.0))
        step = 1
        while step < tokens:
            below = (row // step == col // step + 1) & (lax.rem(row // step, 2) == 1)
            picked = [jnp.where(below, one, 0.0) for one in coupled]
            if step == 1:
                inverse = [same.astype(F32) - one for one in picked]
            else:
                short = [one.astype(BF16) for one in inverse]
                right = [dot(a.astype(BF16), b) for a, b in zip(picked, short)]
                inverse = [
                    one - dot(a, b.astype(BF16)) for one, a, b in zip(inverse, short, right)
                ]
            step = 2 * step
        for (b, h), one in zip(blocks, inverse):
            inverse_ref[b, h] = one

    invert([(member, h) for h in range(held)])
    for name in ("scal", "keys"):
        for p in range(1, size):
            swaps[name, p].wait_recv()
    if size > 1:
        invert(
            [(lax.rem(member - p + size, size), h) for p in range(1, size) for h in range(held)]
        )
    for p in range(1, size):
        swaps["values", p].wait_recv()
    pieces = [(b, h) for b in range(size) for h in range(held)]
    facts_of, updates, steps = {}, {}, {}
    for b, h in pieces:
        tile = scal_in[b, h]
        norm_row = norm_ref[b, h][0:1]
        tile = jnp.where(slot == 3, norm_row, tile)
        columns = columns_of(tile)
        before = scal_in[b - 1, h][2:3, tokens - 1 :] if b else tile[2:3, 0:1]
        last_label, last_sum = tile[2:3, tokens - 1 :], tile[1:2, tokens - 1 :]
        growth_row = jnp.exp(tile[1:2]) * (tile[2:3] == before).astype(F32)
        growth_col = jnp.exp(columns[:, 1:2]) * (columns[:, 2:3] == before).astype(F32)
        tail = jnp.exp(last_sum - columns[:, 1:2]) * (columns[:, 2:3] == last_label).astype(F32)
        fade = jnp.exp(last_sum) * (last_label == before).astype(F32)
        inverse = inverse_ref[b, h]
        keys = r.keys_in[b, :, h * DK : (h + 1) * DK]
        values = r.values_in[b, :, h * DV : (h + 1) * DV]
        update = dot((inverse * tile[0:1]).astype(BF16), values)
        correct = dot((inverse * (tile[0:1] * norm_row * growth_row)).astype(BF16), keys)
        both = jnp.concatenate([update, correct], 1)
        updates[b, h] = both.astype(BF16)
        made = dot_tn(keys, (both * (tail * columns[:, 3:4])).astype(BF16))
        steps[b, h] = (made[:, :DV], made[:, DV:], fade)
        facts_of[b, h] = (growth_col, norm_row)
    built, landed = r.built, r.landed
    rounds = len(hops)
    entry = {}
    summary = {}
    for h in range(held):
        add, erase, fade = steps[0, h]
        carry = jnp.concatenate([jnp.where(same, fade, 0.0) - erase, add], 1)
        for b in range(1, size):
            entry[b, h] = carry.astype(BF16)
            add, erase, fade = steps[b, h]
            carry = fade * carry - dot(erase.astype(BF16), entry[b, h])
            carry = jnp.concatenate([carry[:, :DK], carry[:, DK:] + add], 1)
        summary[h] = carry

    def copy_to_group(source, target, sems, hop):
        return pltpu.make_async_remote_copy(
            src_ref=source,
            dst_ref=target,
            send_sem=sems[0],
            recv_sem=sems[1],
            device_id={"sp": lax.rem(sp + hop * size, ns)},
            device_id_type=MESH,
        )

    def scan_copy(index):
        last = index == rounds - 1
        source, target = built.at[index], landed.at[index]
        if last:
            source, target = source.at[1], target.at[1]
        sems = r.scan_sem.at[0, index], r.scan_sem.at[1, index]
        return copy_to_group(source, target, sems, hops[index])

    note = None
    if groups_all > 1:
        note = copy_to_group(
            scal_in.at[size - 1, 0],
            r.label_note,
            (r.note_sem.at[0], r.note_sem.at[1]),
            1,
        )
        note.start()
        for h in range(held):
            built[0, 1, h] = summary[h][:, DK:].astype(BF16)
    single = rounds == 1
    if groups_all > 1 and single:

        @pl.when(group + hops[0] < groups_all)
        def _():
            scan_copy(0).start()

    for p in range(1, size):
        swaps["queries", p].wait_recv()
    for b, h in pieces:
        growth_col, norm_row = facts_of[b, h]
        keys = r.keys_in[b, :, h * DK : (h + 1) * DK]
        queries = r.queries_in[b, :, h * DK : (h + 1) * DK]
        wide = queries.astype(F32)
        scale = lax.rsqrt(jnp.sum(wide * wide, 1, keepdims=True) + 1e-06) * DK ** (-0.5)
        scores = (dot_nt(queries, keys) * scale * norm_row * decay_ref[b, h]).astype(BF16)
        seen = dot(scores, updates[b, h])
        grown = wide * (scale * growth_col) - seen[:, DV:]
        rows_here = pl.ds(b * tokens, tokens)
        if b:
            carried = dot(grown.astype(BF16), entry[b, h])
            r.reader[h, rows_here] = carried[:, :DK].astype(BF16)
            r.partial[h, rows_here] = seen[:, :DV] + carried[:, DK:]
        else:
            r.reader[h, rows_here] = grown.astype(BF16)
            r.partial[h, rows_here] = seen[:, :DV]
    incoming = None
    if groups_all > 1:
        note.wait_recv()
        joined = (r.label_note[2:3, tokens - 1 :] == scal_in[0, 0][2:3, 0:1]) & (group > 0)
        joined = joined.astype(F32)
        window = None
        if not single:
            for h in range(held):
                built[0, 0, h] = (summary[h][:, :DK] * joined).astype(BF16)
        for index, hop in enumerate(hops):
            last = index == rounds - 1
            if not single:

                @pl.when(group + hop < groups_all)
                def _():
                    scan_copy(index).start()

            @pl.when(group >= hop)
            def _():
                scan_copy(index).wait_recv()

            @pl.when(group < hop)
            def _():
                landed[index] = jnp.zeros_like(landed[index])

            got = landed.at[index]
            if index == 0:
                if last:
                    incoming = [got[1, h].astype(F32) * joined for h in range(held)]
                else:
                    for h in range(held):
                        built[1, 0, h] = dot(built[0, 0, h], got[0, h]).astype(BF16)
                        built[1, 1, h] = (
                            dot(built[0, 0, h], got[1, h]) + built[0, 1, h].astype(F32)
                        ).astype(BF16)
                window = got
            else:
                shifts = [
                    dot(window[0, h], got[1, h]) + window[1, h].astype(F32) for h in range(held)
                ]
                if last:
                    incoming = [one * joined for one in shifts]
                else:
                    for h in range(held):
                        built[index + 1, 0, h] = dot(window[0, h], got[0, h]).astype(BF16)
                        built[index + 1, 1, h] = shifts[h].astype(BF16)
                    window = built.at[index + 1]
    for p in range(1, size):
        swaps["gate", p].wait_recv()
    for h in range(held):
        mixed = r.partial[h]
        if incoming is not None:
            mixed = mixed + dot(r.reader[h], incoming[h].astype(BF16))
        mixed = mixed * lax.rsqrt(jnp.mean(mixed * mixed, -1, keepdims=True) + 1e-06)
        for b in range(size):
            gate = r.gate_in[b, :, h * DV : (h + 1) * DV].astype(F32)
            here = mixed[b * tokens : (b + 1) * tokens] * (gate / (1.0 + jnp.exp(-gate)))
            r.mixed[b, :, h * DV : (h + 1) * DV] = here.astype(BF16)
    gives = []
    for p in range(1, size):
        other = lax.rem(member + p, size)
        gives.append(
            send(
                r.mixed.at[other],
                part_of(r.heads, member),
                r.give_sem,
                (p - 1,),
                {"sp": first + other},
            )
        )
    part_of(r.heads, member)[...] = r.mixed[member]
    for copy in gives:
        copy.wait_recv()
    loads[0].wait()

    def head_block(t):
        start = pl.multiple_of(t * width, width)
        return dot(r.heads[...], r.wo[:, pl.ds(start, width)])

    far_first = list(range(1, chips)) + [0]
    head_pairs, head_across = {}, []
    for k in far_first:
        r.head_out[k] = head_block(2 * lax.rem(chip + k, chips) + 1 - core).astype(BF16)
        head_pairs[k] = send(
            r.head_out.at[k], r.head_in.at[k], r.head_sem, (k,), {"tp": partner}
        )
    for k in far_first:
        there = 2 * lax.rem(chip + k, chips) + core
        value = head_block(there)
        head_pairs[k].wait_recv()
        value = value + r.head_in[k].astype(F32)
        if k:
            r.head_yout[k - 1] = value.astype(BF16)
            head_across.append(
                send(
                    r.head_yout.at[k - 1],
                    r.head_yin.at[k - 1],
                    r.head_sem,
                    (chips + k - 1,),
                    {"tp": there},
                )
            )
    projected = value + ALPHA * r.rows[...].astype(F32)
    for k, copy in enumerate(head_across):
        copy.wait_recv()
        projected = projected + r.head_yin[k].astype(F32)

    picked = dot(r.pick[...], projected.astype(BF16)).astype(BF16)
    sbuf, gathered = r.sbuf, r.gathered
    for e in range(experts):
        sbuf[e] = picked[e * pad : e * pad + cap]
    arrivals = {}
    for i, hop in enumerate(order):
        if hop:
            to = lax.rem(sp + hop, ns)
            arrivals[i] = send(sbuf.at[to], gathered.at[tp, i], r.sp_sem, (i,), {"sp": to})
    gathered[tp, 0] = sbuf[sp]

    def stats_start(index, summed):
        r.stat_own[index] = row_stats(summed)
        return [
            send(
                r.stat_own.at[index],
                r.stat_in.at[index, hop - 1],
                r.stat_sem,
                (index, hop - 1),
                {"tp": lax.rem(tp + hop, nt)},
            )
            for hop in range(1, nt)
        ]

    def stats_end(index, copies, summed, gain):
        total = r.stat_own[index]
        for hop in range(1, nt):
            copies[hop - 1].wait_recv()
            total = total + r.stat_in[index, hop - 1]
        total = columns_of(total / (width * nt))
        mean, square = total[:, 0:1], total[:, 1:2]
        return (summed - mean) * lax.rsqrt(square - mean * mean + 1e-05) * gain

    across, forward = {}, {}

    def arrive(c):
        for i in range(bounds[c], bounds[c + 1]):
            if order[i]:
                arrivals[i].wait_recv()
            mine = gathered.at[tp, i]
            for k in range(1, chips):
                across[i, k] = send(
                    mine, mine, r.y_sem, (i, k - 1),
                    {"tp": 2 * lax.rem(chip + k, chips) + core},
                )
            forward[i, 0] = send(mine, mine, r.pair_sem, (i, 0), {"tp": partner})

    def relay(c):
        for i in range(bounds[c], bounds[c + 1]):
            for k in range(1, chips):
                across[i, k].wait_recv()
                theirs = gathered.at[2 * lax.rem(chip - k + chips, chips) + core, i]
                forward[i, k] = send(theirs, theirs, r.pair_sem, (i, k), {"tp": partner})

    def assemble(c):
        for i in range(bounds[c], bounds[c + 1]):
            for k in range(chips):
                forward[i, k].wait_recv()
            if order[i]:
                notes[i].wait_recv()
            r.side[i * pad : (i + 1) * pad] = columns_of(infos[i])[:pad]
            blocks = [gathered[t, i].astype(F32) for t in range(nt)]
            total = functools.reduce(jnp.add, blocks)
            mean = jnp.sum(total, 1, keepdims=True) / (width * nt)
            blocks = [one - mean for one in blocks]
            square = functools.reduce(jnp.add, [one * one for one in blocks])
            scale = lax.rsqrt(jnp.sum(square, 1, keepdims=True) / (width * nt) + 1e-05)
            for t in range(nt):
                r.inputs[i * pad : i * pad + cap, t * width : (t + 1) * width] = (
                    blocks[t] * scale * gain_in[t][0:1]
                ).astype(BF16)

    tile = 256 if units % 256 == 0 else 128
    silu = jax.nn.silu

    def expert(c):
        rows_here = slice(bounds[c] * pad, bounds[c + 1] * pad)
        inputs = r.inputs
        weight_e, shared_e = r.side[rows_here, 0:1], r.side[rows_here, 1:2]
        if joint:
            both = dot(inputs[rows_here], r.cvr[...])
            gate, up = both[:, :narrow], both[:, narrow:]
        else:
            gate = dot(inputs[rows_here], r.cvr[0])
            up = dot(inputs[rows_here], r.cvr[1])
        r.hidden[rows_here, units:] = (silu(gate) * up * shared_e).astype(BF16)

        @pl.loop(0, units // tile)
        def _(i):
            cols = pl.ds(pl.multiple_of(i * tile, tile), tile)
            gate = dot(inputs[rows_here], r.wv[:, cols])
            up = dot(inputs[rows_here], r.wr[:, cols])
            r.hidden[rows_here, cols] = (silu(gate) * up * weight_e).astype(BF16)

    def part_block(c, t):
        rows_here = slice(bounds[c] * pad, bounds[c + 1] * pad)
        cols = pl.ds(pl.multiple_of(t * width, width), width)
        return dot(r.hidden[rows_here], hid_w[:, cols])

    part_pairs, part_across, backs = {}, {}, {}

    def lower(c):
        low, top = bounds[c], bounds[c + 1]
        for k in far_first:
            value = part_block(c, 2 * lax.rem(chip + k, chips) + 1 - core).astype(BF16)
            for i in range(low, top):
                r.part_out[k, i] = value[(i - low) * pad : (i - low) * pad + cap]
            part_pairs[k] = send(
                r.part_out.at[k, low:top], r.part_in.at[k, low:top], r.part_sem, (c, k),
                {"tp": partner},
            )
        for k in far_first:
            there = 2 * lax.rem(chip + k, chips) + core
            value = part_block(c, there)
            part_pairs[k].wait_recv()
            for i in reversed(range(low, top)):
                piece = value[(i - low) * pad : (i - low) * pad + cap]
                piece = piece + r.part_in[k, i].astype(F32)
                if k:
                    r.part_yout[k - 1, i] = piece.astype(BF16)
                    part_across[k, i] = send(
                        r.part_yout.at[k - 1, i], r.part_yin.at[k - 1, i], r.fold_sem,
                        (i, k - 1), {"tp": there},
                    )
                else:
                    r.own[i] = piece

    def give_back(c):
        for i in reversed(range(bounds[c], bounds[c + 1])):
            piece = r.own[i]
            for k in range(1, chips):
                part_across[k, i].wait_recv()
                piece = piece + r.part_yin[k - 1, i].astype(F32)
            r.back_out[i] = piece.astype(BF16)
            if order[i]:
                to = lax.rem(sp - order[i] + ns, ns)
                backs[i] = send(
                    r.back_out.at[i], r.back_in.at[sp], r.back_sem, (i,), {"sp": to}
                )
            else:
                r.back_in[sp] = r.back_out[i]

    chunks = len(bounds) - 1
    for c in range(chunks):
        arrive(c)
    relay(0)
    first_stats = stats_start(0, projected)
    for copy in gain_copies:
        copy.wait_recv()
    for load in loads[1:5]:
        load.wait()
    for c in range(chunks):
        assemble(c)
        expert(c)
        if c + 1 < chunks:
            relay(c + 1)
        if c:
            give_back(c - 1)
        else:
            for load in loads[5:]:
                load.wait()
        lower(c)
    give_back(chunks - 1)
    middle = stats_end(0, first_stats, projected, r.gain[...]).astype(BF16)
    for i in backs:
        backs[i].wait_recv()
    for j in range(ns):
        r.returned[j * pad : j * pad + cap] = r.back_in[j]
    second = ALPHA * middle.astype(F32) + dot(r.pick_t[...], r.returned[...])
    copies = stats_start(1, second)
    out_ref[...] = stats_end(1, copies, second, r.last_gain[...]).astype(out_ref.dtype)
    if groups_all > 1:
        for index, hop in enumerate(hops):

            @pl.when(group + hop < groups_all)
            def _():
                scan_copy(index).wait_send()

        note.wait_send()
    for copy in waits:
        copy.wait_send()


def shards(
    probe_vectors,
    address_vectors,
    content_vectors,
    storage_raw_signal,
    fade_raw_signal,
    channel_fade_exponent,
    extra_fade_amount,
    sequence_label,
    exit_valve_raw_signal,
    final_projection_matrix,
    incoming_rows_matrix,
    initial_rescale_factor,
    specialist_picks,
    picked_specialist_share,
    specialist_valve_matrix,
    specialist_raising_matrix,
    specialist_lowering_matrix,
    common_valve_matrix,
    common_raising_matrix,
    common_lowering_matrix,
    latter_rescale_factor,
):
    ns, nt = lax.axis_size("sp"), lax.axis_size("tp")
    tokens, width = incoming_rows_matrix.shape
    heads = storage_raw_signal.shape[0]
    experts = specialist_valve_matrix.shape[0] * ns
    top = specialist_picks.shape[1]
    cap = max(2, 9 * tokens * top // (8 * experts))
    pad = -(-cap // 16) * 16
    size = GROUP
    while heads % size or ns % size:
        size //= 2
    held = heads // size
    reach = -(-(DOC_SPAN - 1) // tokens)
    hops = scan_plan(ns // size, -(-reach // size))
    rounds = len(hops)
    units, narrow = specialist_valve_matrix.shape[2], common_valve_matrix.shape[1]
    features = width * nt
    chips = nt // 2
    across = max(chips - 1, 1)
    bounds = (0, 3 * ns // 8, ns)
    swap = max(size - 1, 1)
    dma = pltpu.SemaphoreType.DMA

    def vm(*shape, dtype=BF16):
        return pltpu.VMEM(shape, dtype)

    f32 = functools.partial(vm, dtype=F32)
    operands = dict(
        storage=storage_raw_signal,
        fade=fade_raw_signal,
        fade_exp=channel_fade_exponent[None, :],
        extra=extra_fade_amount,
        label=sequence_label[None, :],
        keys=address_vectors,
        values=content_vectors,
        queries=probe_vectors,
        gate=exit_valve_raw_signal,
        rows=incoming_rows_matrix,
        gain=initial_rescale_factor[None, :],
        last_gain=latter_rescale_factor[None, :],
        picks=specialist_picks.T,
        share=picked_specialist_share.T,
    )
    weights = dict(
        wo_hbm=final_projection_matrix,
        wv_hbm=specialist_valve_matrix,
        wr_hbm=specialist_raising_matrix,
        wd_hbm=specialist_lowering_matrix,
        cv_hbm=common_valve_matrix,
        cr_hbm=common_raising_matrix,
        cd_hbm=common_lowering_matrix,
    )
    shapes = {name: pltpu.VMEM(one.shape, one.dtype) for name, one in operands.items()}
    scratch = dict(
        **shapes,
        take_sem=dma((len(operands),)),
        wo=vm(*final_projection_matrix.shape),
        wv=vm(features, units),
        wr=vm(features, units),
        cvr=vm(features, 2 * narrow) if narrow % 128 == 0 else vm(2, features, narrow),
        wd=vm(units + narrow, features),
        weight_sem=dma((7,)),
        scal_out=f32(heads, 8, tokens),
        scal_in=f32(size, held, 8, tokens),
        keys_in=vm(size, tokens, held * DK),
        values_in=vm(size, tokens, held * DV),
        queries_in=vm(size, tokens, held * DK),
        gate_in=vm(size, tokens, held * DV),
        swap_sem=dma((2, 5, swap)),
        gain_out=f32(8, width),
        gain_in=f32(nt, 8, width),
        gain_sem=dma((2, nt - 1)),
        pick=vm(experts * pad, tokens),
        pick_t=vm(tokens, experts * pad),
        info=f32(experts, 8, 128),
        infos=f32(ns, 8, 128),
        info_sem=dma((2, ns)),
        inverse=f32(size, held, tokens, tokens),
        decay=f32(size, held, tokens, tokens),
        norm=f32(size, held, 8, tokens),
        built=vm(rounds, 2, held, DK, DV),
        landed=vm(rounds, 2, held, DK, DV),
        scan_sem=dma((2, rounds)),
        label_note=f32(8, tokens),
        note_sem=dma((2,)),
        reader=vm(held, size * tokens, DK),
        partial=f32(held, size * tokens, DV),
        mixed=vm(size, tokens, held * DV),
        heads=vm(tokens, heads * DV),
        give_sem=dma((2, swap)),
        head_out=vm(chips, tokens, width),
        head_in=vm(chips, tokens, width),
        head_yout=vm(across, tokens, width),
        head_yin=vm(across, tokens, width),
        head_sem=dma((2, 2 * chips)),
        stat_own=f32(2, 8, tokens),
        stat_in=f32(2, nt - 1, 8, tokens),
        stat_sem=dma((2, 2, nt - 1)),
        sbuf=vm(ns, cap, width),
        gathered=vm(nt, ns, cap, width),
        sp_sem=dma((2, ns)),
        y_sem=dma((2, ns, across)),
        pair_sem=dma((2, ns, chips)),
        inputs=vm(ns * pad, features),
        hidden=vm(ns * pad, units + narrow),
        side=f32(ns * pad, 128),
        part_out=vm(chips, ns, cap, width),
        part_in=vm(chips, ns, cap, width),
        part_yout=vm(across, ns, cap, width),
        part_yin=vm(across, ns, cap, width),
        part_sem=dma((2, len(bounds) - 1, chips)),
        fold_sem=dma((2, ns, across)),
        own=f32(ns, cap, width),
        back_out=vm(ns, cap, width),
        back_in=vm(ns, cap, width),
        back_sem=dma((2, ns)),
        returned=vm(ns * pad, width),
    )
    plan = SimpleNamespace(
        names=tuple(name + "_hbm" for name in operands) + tuple(weights) + ("out",) + tuple(scratch),
        inputs=tuple(operands),
        ns=ns,
        nt=nt,
        cap=cap,
        pad=pad,
        bounds=bounds,
        size=size,
        held=held,
        hops=hops,
    )
    return pl.pallas_call(
        functools.partial(whole_kernel, plan),
        out_shape=jax.ShapeDtypeStruct((tokens, width), BF16),
        in_specs=[pl.BlockSpec(memory_space=pl.ANY)] * (len(operands) + len(weights)),
        out_specs=pl.BlockSpec(memory_space=pltpu.VMEM),
        scratch_shapes=list(scratch.values()),
        compiler_params=pltpu.CompilerParams(
            collective_id=1, has_side_effects=True, vmem_limit_bytes=60 * 2**20
        ),
        name="whole_layer",
    )(*operands.values(), *weights.values())


def solution(mesh):
    placed = (
        P("sp", "tp"),
        P("sp", "tp"),
        P("sp", "tp"),
        P("tp", "sp"),
        P("tp", "sp"),
        P("tp"),
        P("tp", "sp"),
        P("sp"),
        P("sp", "tp"),
        P("tp", None),
        P("sp", "tp"),
        P("tp"),
        P("sp", None),
        P("sp", None),
        P("sp", None, "tp"),
        P("sp", None, "tp"),
        P("sp", "tp", None),
        P(None, "tp"),
        P(None, "tp"),
        P("tp", None),
        P("tp"),
    )
    return jax.shard_map(
        shards, mesh=mesh, in_specs=placed, out_specs=P("sp", "tp"), check_vma=False
    )
```

```python
import functools
from types import SimpleNamespace

import jax
import jax.numpy as jnp
from jax import lax
from jax.experimental import pallas as pl
from jax.experimental.pallas import tpu as pltpu
from jax.sharding import PartitionSpec as P

DK = 128
DV = 128
DOC_SPAN = 768
GROUP = 4

ALPHA = 2.0**0.25
MESH = pl.DeviceIdType.MESH
F32, BF16 = jnp.float32, jnp.bfloat16


def scan_plan(n, reach):
    hops = [1]
    covered = 1
    if reach > 1 and n > 2:
        hops.append(2)
        covered = 3
        while covered < min(reach, n - 1):
            hops.append(covered)
            covered = 2 * covered
    return hops


def hop_order(n):
    order = [0]
    for near in range(1, n // 2 + 1):
        order.append(near)
        if n - near != near:
            order.append(n - near)
    return sorted(order, key=lambda hop: hop % 2)


def dot(left, right):
    return jnp.dot(left, right, preferred_element_type=F32)


def dot_nt(left, right):
    return lax.dot_general(left, right, (((1,), (1,)), ((), ())), preferred_element_type=F32)


def dot_tn(left, right):
    return lax.dot_general(left, right, (((0,), (0,)), ((), ())), preferred_element_type=F32)


def iota(shape, dim):
    return lax.broadcasted_iota(jnp.int32, shape, dim)


def row_stats(array):
    lane = iota((array.shape[0], 128), 1)
    total = jnp.sum(array, -1, keepdims=True)
    square = jnp.sum(array * array, -1, keepdims=True)
    return jnp.where(lane == 0, total, jnp.where(lane == 1, square, 0.0)).T[:8]


def columns_of(rows):
    return jnp.concatenate([rows] * (128 // rows.shape[0]), 0).T


def whole_kernel(plan, *refs):
    r = SimpleNamespace(**dict(zip(plan.names, refs)))
    ns, nt, cap, pad = plan.ns, plan.nt, plan.cap, plan.pad
    size, held, hops = plan.size, plan.held, plan.hops
    order, bounds = hop_order(ns), plan.bounds
    groups_all = ns // size
    sp, tp = lax.axis_index("sp"), lax.axis_index("tp")
    chips = nt // 2
    chip, core = tp // 2, lax.rem(tp, 2)
    partner = tp + 1 - 2 * core
    member, group = lax.rem(sp, size), sp // size
    first = group * size
    out_ref = r.out
    tokens, width = out_ref.shape
    heads = r.storage.shape[0]
    span = held * DK
    units, narrow = r.wv_hbm.shape[2], r.cv_hbm.shape[1]
    joint = narrow % 128 == 0
    experts = ns

    hid_w = r.wd
    pairs = [
        (r.wo_hbm, r.wo),
        (r.wv_hbm.at[0], r.wv),
        (r.wr_hbm.at[0], r.wr),
    ]
    if joint:
        pairs += [
            (r.cv_hbm, r.cvr.at[:, :narrow]),
            (r.cr_hbm, r.cvr.at[:, narrow:]),
        ]
    else:
        pairs += [(r.cv_hbm, r.cvr.at[0]), (r.cr_hbm, r.cvr.at[1])]
    pairs += [(r.wd_hbm.at[0], hid_w.at[:units]), (r.cd_hbm, hid_w.at[units:])]
    loads = [
        pltpu.make_async_copy(source, target, r.weight_sem.at[i])
        for i, (source, target) in enumerate(pairs)
    ]
    takes = {
        name: pltpu.make_async_copy(
            getattr(r, name + "_hbm"), getattr(r, name), r.take_sem.at[i]
        )
        for i, name in enumerate(plan.inputs)
    }
    for take in takes.values():
        take.start()

    def have(*names):
        for name in names or tuple(takes):
            takes.pop(name).wait()
    barrier = pltpu.get_barrier_semaphore()
    for hop in range(1, ns):
        pl.semaphore_signal(
            barrier, inc=1, device_id={"sp": lax.rem(sp + hop, ns)}, device_id_type=MESH
        )
    for hop in range(1, nt):
        pl.semaphore_signal(
            barrier, inc=1, device_id={"tp": lax.rem(tp + hop, nt)}, device_id_type=MESH
        )
    row, col = iota((tokens, tokens), 0), iota((tokens, tokens), 1)
    upper = (row <= col).astype(BF16)
    have("fade_exp", "extra", "fade", "storage", "label", "gain")
    rate = jnp.exp(r.fade_exp[...])
    eye_h = iota((heads, heads), 0) == iota((heads, heads), 1)
    rate = jnp.sum(jnp.where(eye_h, rate, 0.0), 1, keepdims=True)
    decay = r.extra[...] - rate * jnp.log(1.0 + jnp.exp(r.fade[...]))
    write = 1.0 / (1.0 + jnp.exp(-r.storage[...]))
    high = decay.astype(BF16)
    rest = decay - high.astype(F32)
    middle_part = rest.astype(BF16)
    low = (rest - middle_part.astype(F32)).astype(BF16)
    cumulative = dot(high, upper) + dot(middle_part, upper) + dot(low, upper)
    label = r.label[...].astype(F32)
    slot = iota((8, tokens), 0)
    scal_out, scal_in = r.scal_out, r.scal_in
    for h in range(heads):
        tile = jnp.where(slot == 0, write[h : h + 1], 0.0)
        tile = jnp.where(slot == 1, cumulative[h : h + 1], tile)
        scal_out[h] = jnp.where(slot == 2, label, tile)
    r.gain_out[...] = jnp.broadcast_to(r.gain[...], r.gain_out.shape)
    pl.semaphore_wait(barrier, ns - 1 + nt - 1)
    have()
    waits = []

    def send(source, target, sems, place, where):
        copy = pltpu.make_async_remote_copy(
            src_ref=source,
            dst_ref=target,
            send_sem=sems.at[(0,) + place],
            recv_sem=sems.at[(1,) + place],
            device_id=where,
            device_id_type=MESH,
        )
        copy.start()
        waits.append(copy)
        return copy

    def part_of(ref, which):
        return ref.at[:, pl.ds(pl.multiple_of(which * span, 128), span)]

    swaps = {}
    for index, name in enumerate(("scal", "keys", "values", "queries", "gate")):
        for p in range(1, size):
            other = lax.rem(member + p, size)
            if name == "scal":
                source, target = scal_out.at[pl.ds(other * held, held)], scal_in.at[member]
            else:
                source, target = part_of(getattr(r, name), other), getattr(r, name + "_in").at[member]
            swaps[name, p] = send(
                source, target, r.swap_sem, (index, p - 1), {"sp": first + other}
            )
    gain_in = r.gain_in
    gain_copies = [
        send(
            r.gain_out, gain_in.at[tp], r.gain_sem, (hop - 1,), {"tp": lax.rem(tp + hop, nt)}
        )
        for hop in range(1, nt)
    ]
    gain_in[tp] = r.gain_out[...]
    for h in range(held):
        scal_in[member, h] = scal_out[member * held + h]
    for name in ("keys", "values", "queries", "gate"):
        getattr(r, name + "_in")[member] = part_of(getattr(r, name), member)[...]

    for load in loads:
        load.start()
    r.inputs[...] = jnp.zeros_like(r.inputs)
    r.returned[...] = jnp.zeros_like(r.returned)

    pick_rows, share_rows = r.picks[...].astype(F32), r.share[...].astype(F32)
    fact_rows = jnp.where(slot == 0, pick_rows[0:1], 0.0)
    fact_rows = jnp.where(slot == 1, share_rows[0:1], fact_rows)
    fact_rows = jnp.where(slot == 2, share_rows[1:2], fact_rows)
    fact_rows = jnp.where(slot == 3, 1.0, fact_rows)
    pick_cols = columns_of(jnp.where(slot == 4, pick_rows[1:2], fact_rows))
    pick_a, pick_b = pick_cols[:, 0:1], pick_cols[:, 4:5]
    lane = iota((tokens, 128), 1)
    lane_f = lane.astype(F32)
    member_of = ((pick_a == lane_f) | (pick_b == lane_f)).astype(F32)
    strict_low = (row > col).astype(BF16)
    ranks = dot(strict_low, member_of.astype(BF16))
    coded = ((ranks + 1.0) * member_of).astype(BF16)
    slots = experts * pad
    owner = iota((128, slots), 0)
    place = iota((128, slots), 1)
    spread = ((place >= owner * pad) & (place < owner * pad + pad)).astype(BF16)
    column = iota((8, slots), 1).astype(F32)
    expert_of = jnp.floor((column + 0.5) * (1.0 / pad))
    local = column - expert_of * pad + 1.0
    pick_t = (dot(coded, spread) == local[0:1]).astype(F32)
    r.pick_t[...] = pick_t.astype(BF16)
    r.pick[...] = pick_t.T.astype(BF16)
    facts = dot(fact_rows.astype(BF16), pick_t.astype(BF16))
    leads = facts[0:1] == expert_of[0:1]
    slot_weight = jnp.where(leads, facts[1:2], facts[2:3])
    slot_shared = jnp.where(leads, facts[3:4], 0.0)
    side_rows = jnp.where(iota((8, slots), 0) == 0, slot_weight, slot_shared)
    r.info[...] = jnp.zeros_like(r.info)
    for e in range(experts):
        r.info[e, :, 0:pad] = side_rows[:, e * pad : (e + 1) * pad]

    infos, notes = r.infos, {}
    for i, hop in enumerate(order):
        if hop:
            to = lax.rem(sp + hop, ns)
            notes[i] = send(r.info.at[to], infos.at[i], r.info_sem, (i,), {"sp": to})
    infos[0] = r.info[sp]

    same = row == col
    inverse_ref, decay_ref, norm_ref = r.inverse, r.decay, r.norm

    def invert(blocks):
        coupled, inverse = [], []
        for b, h in blocks:
            keys = r.keys_in[b, :, h * DK : (h + 1) * DK]
            gram = dot_nt(keys, keys)
            tile = scal_in[b, h]
            columns = columns_of(tile)
            diagonal = jnp.where(same, gram, 0.0)
            norm_row = lax.rsqrt(jnp.sum(diagonal, 0, keepdims=True) + 1e-06)
            norm_col = lax.rsqrt(jnp.sum(diagonal, 1, keepdims=True) + 1e-06)
            gap = jnp.where(row >= col, columns[:, 1:2] - tile[1:2], 0.0)
            reach = jnp.where(
                (row >= col) & (columns[:, 2:3] == tile[2:3]), jnp.exp(gap), 0.0
            )
            decay_ref[b, h] = reach
            norm_ref[b, h] = jnp.broadcast_to(norm_row, (8, tokens))
            full = gram * (columns[:, 0:1] * norm_col) * norm_row * reach
            coupled.append(jnp.where(row > col, full, 0.0))
        step = 1
        while step < tokens:
            below = (row // step == col // step + 1) & (lax.rem(row // step, 2) == 1)
            picked = [jnp.where(below, one, 0.0) for one in coupled]
            if step == 1:
                inverse = [same.astype(F32) - one for one in picked]
            else:
                short = [one.astype(BF16) for one in inverse]
                right = [dot(a.astype(BF16), b) for a, b in zip(picked, short)]
                inverse = [
                    one - dot(a, b.astype(BF16)) for one, a, b in zip(inverse, short, right)
                ]
            step = 2 * step
        for (b, h), one in zip(blocks, inverse):
            inverse_ref[b, h] = one

    invert([(member, h) for h in range(held)])
    for name in ("scal", "keys"):
        for p in range(1, size):
            swaps[name, p].wait_recv()
    if size > 1:
        invert(
            [(lax.rem(member - p + size, size), h) for p in range(1, size) for h in range(held)]
        )
    for p in range(1, size):
        swaps["values", p].wait_recv()
    pieces = [(b, h) for b in range(size) for h in range(held)]
    facts_of, updates, steps = {}, {}, {}
    for b, h in pieces:
        tile = scal_in[b, h]
        norm_row = norm_ref[b, h][0:1]
        tile = jnp.where(slot == 3, norm_row, tile)
        columns = columns_of(tile)
        before = scal_in[b - 1, h][2:3, tokens - 1 :] if b else tile[2:3, 0:1]
        last_label, last_sum = tile[2:3, tokens - 1 :], tile[1:2, tokens - 1 :]
        growth_row = jnp.exp(tile[1:2]) * (tile[2:3] == before).astype(F32)
        growth_col = jnp.exp(columns[:, 1:2]) * (columns[:, 2:3] == before).astype(F32)
        tail = jnp.exp(last_sum - columns[:, 1:2]) * (columns[:, 2:3] == last_label).astype(F32)
        fade = jnp.exp(last_sum) * (last_label == before).astype(F32)
        inverse = inverse_ref[b, h]
        keys = r.keys_in[b, :, h * DK : (h + 1) * DK]
        values = r.values_in[b, :, h * DV : (h + 1) * DV]
        update = dot((inverse * tile[0:1]).astype(BF16), values)
        correct = dot((inverse * (tile[0:1] * norm_row * growth_row)).astype(BF16), keys)
        both = jnp.concatenate([update, correct], 1)
        updates[b, h] = both.astype(BF16)
        made = dot_tn(keys, (both * (tail * columns[:, 3:4])).astype(BF16))
        steps[b, h] = (made[:, :DV], made[:, DV:], fade)
        facts_of[b, h] = (growth_col, norm_row)
    built, landed = r.built, r.landed
    rounds = len(hops)
    entry = {}
    summary = {}
    for h in range(held):
        add, erase, fade = steps[0, h]
        carry = jnp.concatenate([jnp.where(same, fade, 0.0) - erase, add], 1)
        for b in range(1, size):
            entry[b, h] = carry.astype(BF16)
            add, erase, fade = steps[b, h]
            carry = fade * carry - dot(erase.astype(BF16), entry[b, h])
            carry = jnp.concatenate([carry[:, :DK], carry[:, DK:] + add], 1)
        summary[h] = carry

    def copy_to_group(source, target, sems, hop):
        return pltpu.make_async_remote_copy(
            src_ref=source,
            dst_ref=target,
            send_sem=sems[0],
            recv_sem=sems[1],
            device_id={"sp": lax.rem(sp + hop * size, ns)},
            device_id_type=MESH,
        )

    def scan_copy(index):
        last = index == rounds - 1
        source, target = built.at[index], landed.at[index]
        if last:
            source, target = source.at[1], target.at[1]
        sems = r.scan_sem.at[0, index], r.scan_sem.at[1, index]
        return copy_to_group(source, target, sems, hops[index])

    note = None
    if groups_all > 1:
        note = copy_to_group(
            scal_in.at[size - 1, 0],
            r.label_note,
            (r.note_sem.at[0], r.note_sem.at[1]),
            1,
        )
        note.start()
        for h in range(held):
            built[0, 1, h] = summary[h][:, DK:].astype(BF16)
    single = rounds == 1
    if groups_all > 1 and single:

        @pl.when(group + hops[0] < groups_all)
        def _():
            scan_copy(0).start()

    for p in range(1, size):
        swaps["queries", p].wait_recv()
    for b, h in pieces:
        growth_col, norm_row = facts_of[b, h]
        keys = r.keys_in[b, :, h * DK : (h + 1) * DK]
        queries = r.queries_in[b, :, h * DK : (h + 1) * DK]
        wide = queries.astype(F32)
        scale = lax.rsqrt(jnp.sum(wide * wide, 1, keepdims=True) + 1e-06) * DK ** (-0.5)
        scores = (dot_nt(queries, keys) * scale * norm_row * decay_ref[b, h]).astype(BF16)
        seen = dot(scores, updates[b, h])
        grown = wide * (scale * growth_col) - seen[:, DV:]
        rows_here = pl.ds(b * tokens, tokens)
        if b:
            carried = dot(grown.astype(BF16), entry[b, h])
            r.reader[h, rows_here] = carried[:, :DK].astype(BF16)
            r.partial[h, rows_here] = seen[:, :DV] + carried[:, DK:]
        else:
            r.reader[h, rows_here] = grown.astype(BF16)
            r.partial[h, rows_here] = seen[:, :DV]
    incoming = None
    if groups_all > 1:
        note.wait_recv()
        joined = (r.label_note[2:3, tokens - 1 :] == scal_in[0, 0][2:3, 0:1]) & (group > 0)
        joined = joined.astype(F32)
        window = None
        if not single:
            for h in range(held):
                built[0, 0, h] = (summary[h][:, :DK] * joined).astype(BF16)
        for index, hop in enumerate(hops):
            last = index == rounds - 1
            if not single:

                @pl.when(group + hop < groups_all)
                def _():
                    scan_copy(index).start()

            @pl.when(group >= hop)
            def _():
                scan_copy(index).wait_recv()

            @pl.when(group < hop)
            def _():
                landed[index] = jnp.zeros_like(landed[index])

            got = landed.at[index]
            if index == 0:
                if last:
                    incoming = [got[1, h].astype(F32) * joined for h in range(held)]
                else:
                    for h in range(held):
                        built[1, 0, h] = dot(built[0, 0, h], got[0, h]).astype(BF16)
                        built[1, 1, h] = (
                            dot(built[0, 0, h], got[1, h]) + built[0, 1, h].astype(F32)
                        ).astype(BF16)
                window = got
            else:
                shifts = [
                    dot(window[0, h], got[1, h]) + window[1, h].astype(F32) for h in range(held)
                ]
                if last:
                    incoming = [one * joined for one in shifts]
                else:
                    for h in range(held):
                        built[index + 1, 0, h] = dot(window[0, h], got[0, h]).astype(BF16)
                        built[index + 1, 1, h] = shifts[h].astype(BF16)
                    window = built.at[index + 1]
    for p in range(1, size):
        swaps["gate", p].wait_recv()
    for h in range(held):
        mixed = r.partial[h]
        if incoming is not None:
            mixed = mixed + dot(r.reader[h], incoming[h].astype(BF16))
        mixed = mixed * lax.rsqrt(jnp.mean(mixed * mixed, -1, keepdims=True) + 1e-06)
        for b in range(size):
            gate = r.gate_in[b, :, h * DV : (h + 1) * DV].astype(F32)
            here = mixed[b * tokens : (b + 1) * tokens] * (gate / (1.0 + jnp.exp(-gate)))
            r.mixed[b, :, h * DV : (h + 1) * DV] = here.astype(BF16)
    gives = []
    for p in range(1, size):
        other = lax.rem(member + p, size)
        gives.append(
            send(
                r.mixed.at[other],
                part_of(r.heads, member),
                r.give_sem,
                (p - 1,),
                {"sp": first + other},
            )
        )
    part_of(r.heads, member)[...] = r.mixed[member]
    for copy in gives:
        copy.wait_recv()
    loads[0].wait()

    def head_block(t):
        start = pl.multiple_of(t * width, width)
        return dot(r.heads[...], r.wo[:, pl.ds(start, width)])

    far_first = list(range(1, chips)) + [0]
    head_pairs, head_across = {}, []
    for k in far_first:
        r.head_out[k] = head_block(2 * lax.rem(chip + k, chips) + 1 - core).astype(BF16)
        head_pairs[k] = send(
            r.head_out.at[k], r.head_in.at[k], r.head_sem, (k,), {"tp": partner}
        )
    for k in far_first:
        there = 2 * lax.rem(chip + k, chips) + core
        value = head_block(there)
        head_pairs[k].wait_recv()
        value = value + r.head_in[k].astype(F32)
        if k:
            r.head_yout[k - 1] = value.astype(BF16)
            head_across.append(
                send(
                    r.head_yout.at[k - 1],
                    r.head_yin.at[k - 1],
                    r.head_sem,
                    (chips + k - 1,),
                    {"tp": there},
                )
            )
    projected = value + ALPHA * r.rows[...].astype(F32)
    for k, copy in enumerate(head_across):
        copy.wait_recv()
        projected = projected + r.head_yin[k].astype(F32)

    picked = dot(r.pick[...], projected.astype(BF16)).astype(BF16)
    sbuf, gathered = r.sbuf, r.gathered
    for e in range(experts):
        sbuf[e] = picked[e * pad : e * pad + cap]
    arrivals = {}
    for i, hop in enumerate(order):
        if hop:
            to = lax.rem(sp + hop, ns)
            arrivals[i] = send(sbuf.at[to], gathered.at[tp, i], r.sp_sem, (i,), {"sp": to})
    gathered[tp, 0] = sbuf[sp]

    def stats_start(index, summed):
        r.stat_own[index] = row_stats(summed)
        return [
            send(
                r.stat_own.at[index],
                r.stat_in.at[index, hop - 1],
                r.stat_sem,
                (index, hop - 1),
                {"tp": lax.rem(tp + hop, nt)},
            )
            for hop in range(1, nt)
        ]

    def stats_end(index, copies, summed, gain):
        total = r.stat_own[index]
        for hop in range(1, nt):
            copies[hop - 1].wait_recv()
            total = total + r.stat_in[index, hop - 1]
        total = columns_of(total / (width * nt))
        mean, square = total[:, 0:1], total[:, 1:2]
        return (summed - mean) * lax.rsqrt(square - mean * mean + 1e-05) * gain

    across, forward = {}, {}

    def arrive(c):
        for i in range(bounds[c], bounds[c + 1]):
            if order[i]:
                arrivals[i].wait_recv()
            mine = gathered.at[tp, i]
            for k in range(1, chips):
                across[i, k] = send(
                    mine, mine, r.y_sem, (i, k - 1),
                    {"tp": 2 * lax.rem(chip + k, chips) + core},
                )
            forward[i, 0] = send(mine, mine, r.pair_sem, (i, 0), {"tp": partner})

    def relay(c):
        for i in range(bounds[c], bounds[c + 1]):
            for k in range(1, chips):
                across[i, k].wait_recv()
                theirs = gathered.at[2 * lax.rem(chip - k + chips, chips) + core, i]
                forward[i, k] = send(theirs, theirs, r.pair_sem, (i, k), {"tp": partner})

    def assemble(c):
        for i in range(bounds[c], bounds[c + 1]):
            for k in range(chips):
                forward[i, k].wait_recv()
            if order[i]:
                notes[i].wait_recv()
            r.side[i * pad : (i + 1) * pad] = columns_of(infos[i])[:pad]
            blocks = [gathered[t, i].astype(F32) for t in range(nt)]
            total = functools.reduce(jnp.add, blocks)
            mean = jnp.sum(total, 1, keepdims=True) / (width * nt)
            blocks = [one - mean for one in blocks]
            square = functools.reduce(jnp.add, [one * one for one in blocks])
            scale = lax.rsqrt(jnp.sum(square, 1, keepdims=True) / (width * nt) + 1e-05)
            for t in range(nt):
                r.inputs[i * pad : i * pad + cap, t * width : (t + 1) * width] = (
                    blocks[t] * scale * gain_in[t][0:1]
                ).astype(BF16)

    tile = 256 if units % 256 == 0 else 128
    silu = jax.nn.silu

    def expert(c, after=None):
        rows_here = slice(bounds[c] * pad, bounds[c + 1] * pad)
        inputs = r.inputs
        weight_e, shared_e = r.side[rows_here, 0:1], r.side[rows_here, 1:2]
        if joint:
            both = dot(inputs[rows_here], r.cvr[...])
            gate, up = both[:, :narrow], both[:, narrow:]
        else:
            gate = dot(inputs[rows_here], r.cvr[0])
            up = dot(inputs[rows_here], r.cvr[1])
        r.hidden[rows_here, units:] = (silu(gate) * up * shared_e).astype(BF16)

        for i in range(units // tile):
            cols = slice(i * tile, (i + 1) * tile)
            gate = dot(inputs[rows_here], r.wv[:, cols])
            up = dot(inputs[rows_here], r.wr[:, cols])
            r.hidden[rows_here, cols] = (silu(gate) * up * weight_e).astype(BF16)
            if after is not None and i == (units // tile - 1) // 2:
                after(c - 1)

    def part_block(c, t):
        rows_here = slice(bounds[c] * pad, bounds[c + 1] * pad)
        cols = pl.ds(pl.multiple_of(t * width, width), width)
        return dot(r.hidden[rows_here], hid_w[:, cols])

    part_pairs, part_across, backs = {}, {}, {}

    def lower_pairs(c):
        low, top = bounds[c], bounds[c + 1]
        for k in far_first:
            value = part_block(c, 2 * lax.rem(chip + k, chips) + 1 - core).astype(BF16)
            for i in range(low, top):
                r.part_out[k, i] = value[(i - low) * pad : (i - low) * pad + cap]
            part_pairs[c, k] = send(
                r.part_out.at[k, low:top], r.part_in.at[k, low:top], r.part_sem, (c, k),
                {"tp": partner},
            )

    def lower_own(c):
        low, top = bounds[c], bounds[c + 1]
        for k in far_first:
            there = 2 * lax.rem(chip + k, chips) + core
            value = part_block(c, there)
            part_pairs[c, k].wait_recv()
            for i in reversed(range(low, top)):
                piece = value[(i - low) * pad : (i - low) * pad + cap]
                piece = piece + r.part_in[k, i].astype(F32)
                if k:
                    r.part_yout[k - 1, i] = piece.astype(BF16)
                    part_across[k, i] = send(
                        r.part_yout.at[k - 1, i], r.part_yin.at[k - 1, i], r.fold_sem,
                        (i, k - 1), {"tp": there},
                    )
                else:
                    r.own[i] = piece

    def give_back(c):
        for i in reversed(range(bounds[c], bounds[c + 1])):
            piece = r.own[i]
            for k in range(1, chips):
                part_across[k, i].wait_recv()
                piece = piece + r.part_yin[k - 1, i].astype(F32)
            r.back_out[i] = piece.astype(BF16)
            if order[i]:
                to = lax.rem(sp - order[i] + ns, ns)
                backs[i] = send(
                    r.back_out.at[i], r.back_in.at[sp], r.back_sem, (i,), {"sp": to}
                )
            else:
                r.back_in[sp] = r.back_out[i]

    chunks = len(bounds) - 1
    for c in range(chunks):
        arrive(c)
    relay(0)
    first_stats = stats_start(0, projected)
    for copy in gain_copies:
        copy.wait_recv()
    for load in loads[1:]:
        load.wait()
    for c in range(chunks):
        assemble(c)
        expert(c, lower_own if c else None)
        if c + 1 < chunks:
            relay(c + 1)
        lower_pairs(c)
        if c:
            give_back(c - 1)
    lower_own(chunks - 1)
    give_back(chunks - 1)
    middle = stats_end(0, first_stats, projected, r.gain[...]).astype(BF16)
    for i in backs:
        backs[i].wait_recv()
    for j in range(ns):
        r.returned[j * pad : j * pad + cap] = r.back_in[j]
    second = ALPHA * middle.astype(F32) + dot(r.pick_t[...], r.returned[...])
    copies = stats_start(1, second)
    out_ref[...] = stats_end(1, copies, second, r.last_gain[...]).astype(out_ref.dtype)
    if groups_all > 1:
        for index, hop in enumerate(hops):

            @pl.when(group + hop < groups_all)
            def _():
                scan_copy(index).wait_send()

        note.wait_send()
    for copy in waits:
        copy.wait_send()


def shards(
    probe_vectors,
    address_vectors,
    content_vectors,
    storage_raw_signal,
    fade_raw_signal,
    channel_fade_exponent,
    extra_fade_amount,
    sequence_label,
    exit_valve_raw_signal,
    final_projection_matrix,
    incoming_rows_matrix,
    initial_rescale_factor,
    specialist_picks,
    picked_specialist_share,
    specialist_valve_matrix,
    specialist_raising_matrix,
    specialist_lowering_matrix,
    common_valve_matrix,
    common_raising_matrix,
    common_lowering_matrix,
    latter_rescale_factor,
):
    ns, nt = lax.axis_size("sp"), lax.axis_size("tp")
    tokens, width = incoming_rows_matrix.shape
    heads = storage_raw_signal.shape[0]
    experts = specialist_valve_matrix.shape[0] * ns
    top = specialist_picks.shape[1]
    cap = max(2, 9 * tokens * top // (8 * experts))
    pad = -(-cap // 16) * 16
    size = GROUP
    while heads % size or ns % size:
        size //= 2
    held = heads // size
    reach = -(-(DOC_SPAN - 1) // tokens)
    hops = scan_plan(ns // size, -(-reach // size))
    rounds = len(hops)
    units, narrow = specialist_valve_matrix.shape[2], common_valve_matrix.shape[1]
    features = width * nt
    chips = nt // 2
    across = max(chips - 1, 1)
    bounds = (0, 3 * ns // 8, ns)
    swap = max(size - 1, 1)
    dma = pltpu.SemaphoreType.DMA

    def vm(*shape, dtype=BF16):
        return pltpu.VMEM(shape, dtype)

    f32 = functools.partial(vm, dtype=F32)
    operands = dict(
        storage=storage_raw_signal,
        fade=fade_raw_signal,
        fade_exp=channel_fade_exponent[None, :],
        extra=extra_fade_amount,
        label=sequence_label[None, :],
        keys=address_vectors,
        values=content_vectors,
        queries=probe_vectors,
        gate=exit_valve_raw_signal,
        rows=incoming_rows_matrix,
        gain=initial_rescale_factor[None, :],
        last_gain=latter_rescale_factor[None, :],
        picks=specialist_picks.T,
        share=picked_specialist_share.T,
    )
    weights = dict(
        wo_hbm=final_projection_matrix,
        wv_hbm=specialist_valve_matrix,
        wr_hbm=specialist_raising_matrix,
        wd_hbm=specialist_lowering_matrix,
        cv_hbm=common_valve_matrix,
        cr_hbm=common_raising_matrix,
        cd_hbm=common_lowering_matrix,
    )
    shapes = {name: pltpu.VMEM(one.shape, one.dtype) for name, one in operands.items()}
    scratch = dict(
        **shapes,
        take_sem=dma((len(operands),)),
        wo=vm(*final_projection_matrix.shape),
        wv=vm(features, units),
        wr=vm(features, units),
        cvr=vm(features, 2 * narrow) if narrow % 128 == 0 else vm(2, features, narrow),
        wd=vm(units + narrow, features),
        weight_sem=dma((7,)),
        scal_out=f32(heads, 8, tokens),
        scal_in=f32(size, held, 8, tokens),
        keys_in=vm(size, tokens, held * DK),
        values_in=vm(size, tokens, held * DV),
        queries_in=vm(size, tokens, held * DK),
        gate_in=vm(size, tokens, held * DV),
        swap_sem=dma((2, 5, swap)),
        gain_out=f32(8, width),
        gain_in=f32(nt, 8, width),
        gain_sem=dma((2, nt - 1)),
        pick=vm(experts * pad, tokens),
        pick_t=vm(tokens, experts * pad),
        info=f32(experts, 8, 128),
        infos=f32(ns, 8, 128),
        info_sem=dma((2, ns)),
        inverse=f32(size, held, tokens, tokens),
        decay=f32(size, held, tokens, tokens),
        norm=f32(size, held, 8, tokens),
        built=vm(rounds, 2, held, DK, DV),
        landed=vm(rounds, 2, held, DK, DV),
        scan_sem=dma((2, rounds)),
        label_note=f32(8, tokens),
        note_sem=dma((2,)),
        reader=vm(held, size * tokens, DK),
        partial=f32(held, size * tokens, DV),
        mixed=vm(size, tokens, held * DV),
        heads=vm(tokens, heads * DV),
        give_sem=dma((2, swap)),
        head_out=vm(chips, tokens, width),
        head_in=vm(chips, tokens, width),
        head_yout=vm(across, tokens, width),
        head_yin=vm(across, tokens, width),
        head_sem=dma((2, 2 * chips)),
        stat_own=f32(2, 8, tokens),
        stat_in=f32(2, nt - 1, 8, tokens),
        stat_sem=dma((2, 2, nt - 1)),
        sbuf=vm(ns, cap, width),
        gathered=vm(nt, ns, cap, width),
        sp_sem=dma((2, ns)),
        y_sem=dma((2, ns, across)),
        pair_sem=dma((2, ns, chips)),
        inputs=vm(ns * pad, features),
        hidden=vm(ns * pad, units + narrow),
        side=f32(ns * pad, 128),
        part_out=vm(chips, ns, cap, width),
        part_in=vm(chips, ns, cap, width),
        part_yout=vm(across, ns, cap, width),
        part_yin=vm(across, ns, cap, width),
        part_sem=dma((2, len(bounds) - 1, chips)),
        fold_sem=dma((2, ns, across)),
        own=f32(ns, cap, width),
        back_out=vm(ns, cap, width),
        back_in=vm(ns, cap, width),
        back_sem=dma((2, ns)),
        returned=vm(ns * pad, width),
    )
    plan = SimpleNamespace(
        names=tuple(name + "_hbm" for name in operands) + tuple(weights) + ("out",) + tuple(scratch),
        inputs=tuple(operands),
        ns=ns,
        nt=nt,
        cap=cap,
        pad=pad,
        bounds=bounds,
        size=size,
        held=held,
        hops=hops,
    )
    return pl.pallas_call(
        functools.partial(whole_kernel, plan),
        out_shape=jax.ShapeDtypeStruct((tokens, width), BF16),
        in_specs=[pl.BlockSpec(memory_space=pl.ANY)] * (len(operands) + len(weights)),
        out_specs=pl.BlockSpec(memory_space=pltpu.VMEM),
        scratch_shapes=list(scratch.values()),
        compiler_params=pltpu.CompilerParams(
            collective_id=1, has_side_effects=True, vmem_limit_bytes=60 * 2**20
        ),
        name="whole_layer",
    )(*operands.values(), *weights.values())


def solution(mesh):
    placed = (
        P("sp", "tp"),
        P("sp", "tp"),
        P("sp", "tp"),
        P("tp", "sp"),
        P("tp", "sp"),
        P("tp"),
        P("tp", "sp"),
        P("sp"),
        P("sp", "tp"),
        P("tp", None),
        P("sp", "tp"),
        P("tp"),
        P("sp", None),
        P("sp", None),
        P("sp", None, "tp"),
        P("sp", None, "tp"),
        P("sp", "tp", None),
        P(None, "tp"),
        P(None, "tp"),
        P("tp", None),
        P("tp"),
    )
    return jax.shard_map(
        shards, mesh=mesh, in_specs=placed, out_specs=P("sp", "tp"), check_vma=False
    )
```
